128 devices in a mesh: sp: 64 (over z, y, x), tp: 2 (over core).
Axes of the slice: x: 4, y: 4, z: 4, core: 2. Of those that a mesh axis runs over, the one named last changes fastest.
Arguments:
- residual: bfloat16 [16384, 2048], P(('sp', 'tp')), may hold values from -6 to 6
- queries: bfloat16 [16384, 1152], P('sp', 'tp'), may hold values from -800 to 800
- latent: bfloat16 [16384, 256], P('sp'), may hold values from -6 to 6
- rope_key: bfloat16 [16384, 32], P('sp'), may hold values from -6 to 6
- doc_ids: int32 [16384], P('sp'), may hold values from 0 to 5, never falling along the last dimension, each value on 1 to 8192 neighbouring positions
- latent_to_key: bfloat16 [256, 768], P(None, 'tp'), may hold values from -0.375 to 0.375
- latent_to_value: bfloat16 [256, 768], P(None, 'tp'), may hold values from -0.375 to 0.375
- out_proj: bfloat16 [768, 2048], replicated, may hold values from -0.21875 to 0.21875
- mix_gain: float32 [2048], replicated, may hold values from 0.1 to 1.9
- moe_gain: float32 [2048], replicated, may hold values from 0.1 to 1.9
- expert_ids: int32 [16384, 2], P(('sp', 'tp')), may hold values from 0 to 63, as said below
- route_weight: float32 [16384, 2], P(('sp', 'tp')), may hold values from 0.1 to 1
- gate_weight: bfloat16 [64, 2048, 1024], P('sp', None, 'tp'), may hold values from -0.125 to 0.125
- up_weight: bfloat16 [64, 2048, 1024], P('sp', None, 'tp'), may hold values from -0.125 to 0.125
- down_weight: bfloat16 [64, 1024, 2048], P('sp', 'tp'), may hold values from -0.1875 to 0.1875
Outputs:
- output: bfloat16 [16384, 2048], P(('sp', 'tp'))
The draws below stay inside these ranges and needn't reach their ends.
Inputs may be any that keep to these rules, and one draw needn't show every extreme that they name: `expert_ids`: each row names 2 different experts of one group of 16 consecutive numbers; in each aligned block of 128 rows (the rows of one device) no expert is named more than 8 times, and some expert exactly 8 times.
All inputs are finite; a program needn't handle non-finite values.
Results may differ from the reference program's by a relative error of at most 0.013.
Values may be sent and summed in bfloat16 or wider, within the bound.
A program may use at most 64 MiB of HBM per device.

```python
import math
import jax
import jax.numpy as jnp
import numpy as np
from jax import lax

D = 2048
HEAD_COUNT = 12
UNROTATED_DIM = 64
ROPE = 32
VALUE_ENTRIES = 64
LATENT_RANK = 256
FF = 1024
GROUPS = 4
TOP_K = 2
TOK_DEV = 256
TOKEN_COUNT = 16384
EXPERTS = 64
N_TP = 2


def rope_rows(key):
    drawn = jax.random.normal(jax.random.fold_in(key, 11), (TOKEN_COUNT, ROPE), jnp.float32)
    return jnp.clip(drawn, -6.0, 6.0)


def draw_rope_key(key, part):
    return rope_rows(key).astype(jnp.bfloat16)


def draw_queries(key, part):
    normal_part = jax.random.normal(jax.random.fold_in(key, 12), (TOKEN_COUNT, HEAD_COUNT, UNROTATED_DIM + ROPE), jnp.float32)
    normal_part = jnp.clip(normal_part, -6.0, 6.0)
    return normal_part.reshape(TOKEN_COUNT, HEAD_COUNT * (UNROTATED_DIM + ROPE)).astype(jnp.bfloat16)


def draw_expert_ids(key, part):
    row_count = TOK_DEV // N_TP
    half_rows = row_count // 2
    block_count = TOKEN_COUNT // row_count
    per_group = EXPERTS // GROUPS
    full_group = jax.random.randint(jax.random.fold_in(key, 1), (), 0, GROUPS)
    others = jax.random.randint(jax.random.fold_in(key, 2), (block_count, half_rows), 0, GROUPS - 1)
    others = others + (others >= full_group).astype(jnp.int32)
    group_ids = jnp.concatenate([jnp.full((block_count, half_rows), full_group, jnp.int32), others], axis=1)
    block_keys = jax.random.split(jax.random.fold_in(key, 3), block_count)
    group_ids = jax.vmap(lambda block_key, row_groups: jax.random.permutation(block_key, row_groups))(block_keys, group_ids)
    onehot = (group_ids[..., None] == jnp.arange(GROUPS, dtype=jnp.int32)).astype(jnp.int32)
    earlier = jnp.cumsum(onehot, axis=1) - onehot
    slot_rank = jnp.sum(earlier * onehot, axis=-1)
    offsets = jax.random.randint(jax.random.fold_in(key, 4), (block_count, GROUPS), 0, per_group)
    spacing = jax.random.randint(jax.random.fold_in(key, 5), (block_count, GROUPS), 1, per_group)
    own_offset = jnp.take_along_axis(offsets, group_ids, axis=1)
    own_spacing = jnp.take_along_axis(spacing, group_ids, axis=1)
    first_pick = (slot_rank + own_offset) % per_group
    second_pick = (slot_rank + own_offset + own_spacing) % per_group
    chosen = jnp.stack([group_ids * per_group + first_pick, group_ids * per_group + second_pick], axis=-1)
    return chosen.reshape(TOKEN_COUNT, 2).astype(jnp.int32)


def steps_of(own_key, shape, cuts, least, top_value):
    level, own = 1.0, jax.random.fold_in(own_key, 6)
    for axis_at, blocks in cuts:
        draws = jnp.exp(jax.random.uniform(jax.random.fold_in(own, axis_at), (blocks,), jnp.float32, least / len(cuts), top_value / len(cuts)))
        level = level * jnp.repeat(draws, shape[axis_at] // blocks).reshape([-1 if axis == axis_at else 1 for axis in range(len(shape))])
    return level


def profile(number_of, total, bound, slope):
    weights = [(1 << 20) // math.isqrt(rank ** slope) + 1 for rank in range(2, number_of + 1)]
    spare, counts = total - bound - (number_of - 1), [1] * (number_of - 1)
    while spare > 0:
        free = [i for i in range(number_of - 1) if counts[i] < bound]
        mass, remaining = sum([weights[i] for i in free]), spare
        for i in free:
            extra = min(bound - counts[i], max(1, remaining * weights[i] // mass), spare)
            counts[i] = counts[i] + extra
            spare = spare - extra
    return np.array([bound] + counts)


def uneven_parts(own_key, amount, total, limit, slope):
    if amount == 2:
        one = jax.random.randint(own_key, (), max(1, total - limit), min(limit, total - 1) + 1)
        return jnp.stack([one, total - one])
    tallies = jnp.asarray(profile(amount, total, limit, slope), jnp.int32)
    twos = (amount - 1) // 2
    source_of, sink = tallies[1:1 + 2 * twos:2], tallies[2:2 + 2 * twos:2]
    room = jnp.minimum(source_of - 1, limit - sink)
    moved = jax.random.randint(jax.random.fold_in(own_key, 1), (twos,), 0, 1 << 20) % (room + 1)
    tallies = tallies.at[1:1 + 2 * twos:2].set(source_of - moved).at[2:2 + 2 * twos:2].set(sink + moved)
    return tallies[jax.random.permutation(jax.random.fold_in(own_key, 2), amount)]


def bell_draw(key, extent, scale, most, cuts=(), held_as=jnp.bfloat16):
    values = scale * jax.random.normal(key, extent, jnp.float32)
    if cuts:
        values = values * steps_of(key, extent, cuts, -0.22, 0.18)
    return jnp.clip(values, -most, most).astype(held_as)


def setup_inputs(seed: int = 0) -> dict:
    arg_keys = jax.random.split(jax.random.key(seed), 16)
    return {
        "residual": bell_draw(arg_keys[0], (TOKEN_COUNT, D), 1.0, 6.0, ((0, 128),)),
        "queries": draw_queries(jax.random.fold_in(arg_keys[15], 71), 0),
        "latent": bell_draw(arg_keys[2], (TOKEN_COUNT, LATENT_RANK), 1.0, 6.0, ((0, 64),)),
        "rope_key": draw_rope_key(jax.random.fold_in(arg_keys[15], 71), 0),
        "doc_ids": jnp.searchsorted(jnp.cumsum(uneven_parts(arg_keys[4], 6, TOKEN_COUNT, TOKEN_COUNT // 2, 0)), jnp.arange(TOKEN_COUNT), side="right").astype(jnp.int32),
        "latent_to_key": bell_draw(arg_keys[5], (LATENT_RANK, HEAD_COUNT * UNROTATED_DIM), LATENT_RANK ** -0.5, 0.375, ((1, 2),)),
        "latent_to_value": bell_draw(arg_keys[6], (LATENT_RANK, HEAD_COUNT * VALUE_ENTRIES), LATENT_RANK ** -0.5, 0.375, ((1, 2),)),
        "out_proj": bell_draw(arg_keys[7], (HEAD_COUNT * VALUE_ENTRIES, D), (HEAD_COUNT * VALUE_ENTRIES) ** -0.5, 0.21875),
        "mix_gain": jnp.clip(1.0 + 0.18 * jax.random.normal(arg_keys[8], (D,), jnp.float32), 0.1, 1.9),
        "moe_gain": jnp.clip(1.0 + 0.18 * jax.random.normal(arg_keys[9], (D,), jnp.float32), 0.1, 1.9),
        "expert_ids": draw_expert_ids(jax.random.fold_in(arg_keys[15], 71), 0),
        "route_weight": jnp.clip(0.1 + 0.9 * jax.random.uniform(arg_keys[11], (TOKEN_COUNT, TOP_K), jnp.float32) ** steps_of(arg_keys[11], (TOKEN_COUNT, TOP_K), ((0, 128),), -0.2, 0.2), 0.1, 1.0),
        "gate_weight": bell_draw(arg_keys[12], (EXPERTS, D, FF), D ** -0.5, 0.125, ((0, 64), (2, 2))),
        "up_weight": bell_draw(arg_keys[13], (EXPERTS, D, FF), D ** -0.5, 0.125, ((0, 64), (2, 2))),
        "down_weight": bell_draw(arg_keys[14], (EXPERTS, FF, D), FF ** -0.5, 0.1875, ((0, 64), (1, 2))),
    }


rope_base = 10000.0
epsilon = 1e-06
query_rows = 256

def rotate(source, positions):
    half_width = source.shape[-1] // 2
    frequency = rope_base ** (-jnp.arange(half_width, dtype=jnp.float32) / half_width)
    angles = positions.astype(jnp.float32)[:, None] * frequency[None, :]
    if source.ndim == 3:
        angles = angles[:, None, :]
    cosine = jnp.cos(angles)
    sine_part = jnp.sin(angles)
    upper_half = source[..., :half_width].astype(jnp.float32)
    lower_half = source[..., half_width:].astype(jnp.float32)
    turned = jnp.concatenate([upper_half * cosine - lower_half * sine_part, lower_half * cosine + upper_half * sine_part], axis=-1)
    return turned.astype(jnp.bfloat16)

def rms_scale(source, gain):
    return source * lax.rsqrt(lax.optimization_barrier(jnp.mean(source * source, axis=-1, keepdims=True)) + epsilon) * gain

def reference(residual, queries, latent, rope_key, doc_ids, latent_to_key, latent_to_value, out_proj, mix_gain, moe_gain, expert_ids, route_weight, gate_weight, up_weight, down_weight):
    positions = jnp.arange(TOKEN_COUNT, dtype=jnp.int32)
    key_nope = jnp.dot(latent, latent_to_key, preferred_element_type=jnp.float32).astype(jnp.bfloat16)
    key_nope = key_nope.reshape(TOKEN_COUNT, HEAD_COUNT, UNROTATED_DIM).astype(jnp.float32)
    values = jnp.dot(latent, latent_to_value, preferred_element_type=jnp.float32).astype(jnp.bfloat16)
    values = values.reshape(TOKEN_COUNT, HEAD_COUNT, VALUE_ENTRIES).astype(jnp.float32)
    key_rot = rotate(rope_key, positions).astype(jnp.float32)
    shaped = queries.reshape(TOKEN_COUNT, HEAD_COUNT, UNROTATED_DIM + ROPE)
    query_nope = shaped[..., :UNROTATED_DIM]
    query_rot = rotate(shaped[..., UNROTATED_DIM:], positions)
    score_scale = (UNROTATED_DIM + ROPE) ** (-0.5)
    block_count = TOKEN_COUNT // query_rows

    def attend_rows(bundle):
        nope_block, rot_block, pos_block, doc_block = bundle
        scores = (jnp.einsum('qhd,khd->qhk', nope_block.astype(jnp.float32), key_nope) + jnp.einsum('qhr,kr->qhk', rot_block.astype(jnp.float32), key_rot)) * score_scale
        allowed = ((positions[None, :] <= pos_block[:, None]) & (doc_ids[None, :] == doc_block[:, None]))[:, None, :]
        row_max = lax.optimization_barrier(jnp.max(jnp.where(allowed, scores, -jnp.inf), axis=-1, keepdims=True))
        weights = jnp.where(allowed, jnp.exp(scores - row_max), 0.0)
        totals = lax.optimization_barrier(jnp.sum(weights, axis=-1))
        rounded = lax.optimization_barrier(weights.astype(jnp.bfloat16)).astype(jnp.float32)
        mixed = jnp.einsum('qhk,khd->qhd', rounded, values) / totals[..., None]
        return mixed.astype(jnp.bfloat16).reshape(query_rows, HEAD_COUNT * VALUE_ENTRIES)
    attended = lax.map(attend_rows, (query_nope.reshape(block_count, query_rows, HEAD_COUNT, UNROTATED_DIM), query_rot.reshape(block_count, query_rows, HEAD_COUNT, ROPE), positions.reshape(block_count, query_rows), doc_ids.reshape(block_count, query_rows)))
    attended = attended.reshape(TOKEN_COUNT, HEAD_COUNT * VALUE_ENTRIES)
    mix = jnp.dot(attended, out_proj, preferred_element_type=jnp.float32)
    branch = rms_scale(mix, mix_gain)
    middle = lax.optimization_barrier((residual.astype(jnp.float32) + branch).astype(jnp.bfloat16))
    normed = rms_scale(middle.astype(jnp.float32), moe_gain).astype(jnp.bfloat16)
    row_count = TOK_DEV // N_TP
    groups_blocks = TOKEN_COUNT // row_count
    per_group = EXPERTS // GROUPS
    capacity = row_count // per_group
    flat_ids = expert_ids.reshape(groups_blocks, row_count * TOP_K)
    onehot = (flat_ids[..., None] == jnp.arange(EXPERTS, dtype=jnp.int32)).astype(jnp.int32)
    earlier = jnp.cumsum(onehot, axis=1) - onehot
    slot_rank = lax.optimization_barrier(jnp.sum(earlier * onehot, axis=-1)).astype(jnp.int32)
    block_index = jnp.broadcast_to(jnp.arange(groups_blocks, dtype=jnp.int32)[:, None], flat_ids.shape)
    token_index = (block_index * row_count + jnp.arange(row_count * TOP_K, dtype=jnp.int32)[None, :] // TOP_K).astype(jnp.int32)
    row_table = jnp.full((EXPERTS, groups_blocks, capacity), TOKEN_COUNT, jnp.int32)
    row_table = row_table.at[flat_ids, block_index, slot_rank].set(token_index)
    weight_table = jnp.zeros((EXPERTS, groups_blocks, capacity), jnp.float32)
    weight_table = weight_table.at[flat_ids, block_index, slot_rank].set(route_weight.reshape(groups_blocks, row_count * TOP_K))
    padded = jnp.concatenate([normed, jnp.zeros((1, D), jnp.bfloat16)], axis=0)
    half_units = FF // N_TP

    def expert_step(accumulated, inputs):
        table_rows, table_weights, gate_mat, up_mat, down_mat = inputs
        picked = padded[table_rows.reshape(-1)]
        gate_out = jnp.dot(picked, gate_mat, preferred_element_type=jnp.float32)
        up_out = jnp.dot(picked, up_mat, preferred_element_type=jnp.float32)
        hidden = (jax.nn.silu(gate_out) * up_out).astype(jnp.bfloat16)
        combined = jnp.zeros((picked.shape[0], D), jnp.float32)
        for portion in range(N_TP):
            partial_value = jnp.dot(hidden[:, portion * half_units:(portion + 1) * half_units], down_mat[portion * half_units:(portion + 1) * half_units], preferred_element_type=jnp.float32)
            combined = combined + lax.optimization_barrier(partial_value.astype(jnp.bfloat16)).astype(jnp.float32)
        result = lax.optimization_barrier(combined.astype(jnp.bfloat16)).astype(jnp.float32)
        accumulated = accumulated.at[table_rows.reshape(-1)].add(result * table_weights.reshape(-1)[:, None])
        return (accumulated, None)
    accumulated, _ = lax.scan(expert_step, jnp.zeros((TOKEN_COUNT + 1, D), jnp.float32), (row_table, weight_table, gate_weight, up_weight, down_weight))
    return (middle.astype(jnp.float32) + accumulated[:TOKEN_COUNT]).astype(jnp.bfloat16)
```

```python
import functools

import jax
import jax.numpy as jnp
from jax import lax
from jax.experimental import pallas as pl
from jax.experimental.pallas import tpu as pltpu
from jax.sharding import PartitionSpec as P

D = 2048
UNROTATED_DIM = 64
ROPE = 32
HEADS = 6
LATENT = 256
ROWS = 256
HALF = 128
PIECE = 160
EXPERTS = 64
CAP = 8
FF_HALF = 512
PLANE = 16
DEPTH = 4
rope_base = 10000.0
epsilon = 1e-06
MASKED = 1e30
SCORE_BASE2 = float((UNROTATED_DIM + ROPE) ** (-0.5) * 1.4426950408889634)
MESH = pl.DeviceIdType.MESH


def rotate(source, cosine, sine_part):
    half_width = source.shape[-1] // 2
    upper_half = source[..., :half_width].astype(jnp.float32)
    lower_half = source[..., half_width:].astype(jnp.float32)
    turned = jnp.concatenate(
        [
            upper_half * cosine - lower_half * sine_part,
            lower_half * cosine + upper_half * sine_part,
        ],
        axis=-1,
    )
    return turned.astype(jnp.bfloat16)


def nn(a, b):
    return lax.dot_general(a, b, (((1,), (0,)), ((), ())), preferred_element_type=jnp.float32)


def nt(a, b):
    return lax.dot_general(a, b, (((1,), (1,)), ((), ())), preferred_element_type=jnp.float32)


def kernel(
    query_ref,
    own_ref,
    key_w_ref,
    value_w_ref,
    residual_ref,
    mix_gain_ref,
    moe_gain_ref,
    ids_ref,
    ids_t_ref,
    route_ref,
    proj_hbm,
    gate_hbm,
    up_hbm,
    down_hbm,
    out_ref,
    kv,
    run_max,
    run_sum,
    run_out,
    turned_out,
    heads_buf,
    proj,
    gate_w,
    up_w,
    down_w,
    mix,
    middle,
    normed,
    send_buf,
    recv_buf,
    done_buf,
    back_buf,
    z_send,
    plane_send,
    pass_send,
    got,
    passed,
    weight_local,
    weight_send,
    weight_got,
    heads_send,
    heads_got,
    go_send,
    go_got,
    own_copy,
    back_send,
    back_got,
):
    sp = lax.axis_index("sp")
    tp = lax.axis_index("tp")
    other = 1 - tp
    z = sp // PLANE
    me = sp % PLANE

    def remote(src, dst, send_sem, recv_sem, device):
        return pltpu.make_async_remote_copy(
            src_ref=src,
            dst_ref=dst,
            send_sem=send_sem,
            recv_sem=recv_sem,
            device_id=device,
            device_id_type=MESH,
        )

    barrier = pltpu.get_barrier_semaphore()
    pl.semaphore_signal(barrier, inc=1, device_id=(sp, other), device_id_type=MESH)

    def greet(step, carry):
        pl.semaphore_signal(
            barrier, inc=1, device_id=((sp + step) % EXPERTS, tp), device_id_type=MESH
        )
        return carry

    lax.fori_loop(1, EXPERTS, greet, 0)

    local_copies = [
        pltpu.make_async_copy(proj_hbm, proj, weight_local.at[0]),
        pltpu.make_async_copy(gate_hbm.at[0], gate_w.at[tp], weight_local.at[1]),
        pltpu.make_async_copy(up_hbm.at[0], up_w.at[tp], weight_local.at[2]),
        pltpu.make_async_copy(down_hbm.at[0], down_w.at[tp], weight_local.at[3]),
    ]
    for copy in local_copies:
        copy.start()

    pl.semaphore_wait(barrier, EXPERTS)

    next_z = []
    for hop in (1, 2):
        target = ((z + hop) % DEPTH) * PLANE + me
        copy = remote(
            own_ref.at[tp],
            kv.at[hop - 1, me, tp],
            z_send.at[hop - 1],
            got.at[hop - 1, me],
            (target, tp),
        )
        copy.start()
        next_z.append(copy)

    def plane_copy(kind, step, own):
        peer = (me + step) % PLANE
        return remote(
            own_ref.at[tp] if own else kv.at[kind, me, tp],
            kv.at[kind, me, tp],
            plane_send.at[kind, step],
            got.at[kind, me],
            (z * PLANE + peer, tp),
        )

    def send_own(step, carry):
        @pl.when((me + step) % PLANE > me)
        def _():
            plane_copy(1, step, True).start()

        return carry

    lax.fori_loop(1, PLANE, send_own, 0)

    weight_copies = [
        remote(src.at[0], dst.at[tp], weight_send.at[i], weight_got.at[i], (sp, other))
        for i, (src, dst) in enumerate(((gate_hbm, gate_w), (up_hbm, up_w), (down_hbm, down_w)))
    ]
    for copy in weight_copies:
        copy.start()

    lane = lax.broadcasted_iota(jnp.int32, (ROWS, 128), 1)
    low_lanes = lane < 64

    def attend(first, second, causal):
        rows = jnp.concatenate([first[:HALF, :], second[:HALF, :]], axis=0)
        low, high = [], []
        for half in (first, second):
            extra = half[HALF:PIECE, :].astype(jnp.float32)
            for tile in (extra[:, :128], extra[:, 128:]):
                swapped = pltpu.roll(tile, 64, 1)
                low += [tile, swapped]
                high += [swapped, tile]
        low = jnp.concatenate(low, axis=0).astype(jnp.bfloat16)
        high = jnp.concatenate(high, axis=0).astype(jnp.bfloat16)
        keys = nn(rows, key_w_ref[...]).astype(jnp.bfloat16)
        values = nt(value_w_ref[...], rows).astype(jnp.bfloat16)
        for head in range(HEADS):
            column = keys[:, 128 * (head // 2) : 128 * (head // 2) + 128]
            if head % 2 == 0:
                full_key = jnp.where(low_lanes, column, high)
            else:
                full_key = jnp.where(low_lanes, low, column)
            scores = nn(full_key, query_ref[head])
            if causal:
                key_at = lax.broadcasted_iota(jnp.int32, (ROWS, ROWS), 0)
                query_at = lax.broadcasted_iota(jnp.int32, (ROWS, ROWS), 1)
                scores = jnp.where(key_at <= query_at, scores, -MASKED)
                new_max = jnp.max(scores, axis=0, keepdims=True)
            else:
                old_max = run_max[head]
                new_max = jnp.maximum(old_max, jnp.max(scores, axis=0, keepdims=True))
            weights = jnp.exp2((scores - new_max) * SCORE_BASE2)
            sums = jnp.sum(weights.reshape(ROWS // 8, 8, ROWS), axis=0)
            part = nn(values[64 * head : 64 * head + 64, :], weights.astype(jnp.bfloat16))
            if causal:
                run_sum[head] = sums
                run_out[head] = part
            else:
                factor = jnp.exp2((old_max - new_max) * SCORE_BASE2)
                run_sum[head] = run_sum[head] * factor + sums
                run_out[head] = run_out[head] * factor + part
            run_max[head] = new_max

    attend(own_ref.at[0], own_ref.at[1], True)

    def pass_copy(kind, source):
        return remote(
            kv.at[kind, source, tp],
            kv.at[kind, source, tp],
            pass_send.at[kind, source],
            passed.at[kind, source],
            (sp, other),
        )

    def arrival(kind, source):
        return pltpu.make_async_copy(
            kv.at[kind, source, tp], kv.at[kind, source, tp], got.at[kind, source]
        )

    arrival(0, me).wait()
    pass_copy(0, me).start()

    def send_first(step, carry):
        plane_copy(0, step, False).start()
        return carry

    lax.fori_loop(1, PLANE, send_first, 0)
    arrival(1, me).wait()
    pass_copy(1, me).start()

    def send_second(step, carry):
        @pl.when((me + step) % PLANE < me)
        def _():
            plane_copy(1, step, False).start()

        return carry

    lax.fori_loop(1, PLANE, send_second, 0)

    def visit(number, carry):
        step = number // 2
        kind = number % 2
        source = (me - step + PLANE) % PLANE

        later = number + 2

        @pl.when(later < 2 * PLANE)
        def _():
            later_source = (me - later // 2 + PLANE) % PLANE
            arrival(kind, later_source).wait()
            pass_copy(kind, later_source).start()

        pltpu.make_async_copy(
            kv.at[kind, source, other], kv.at[kind, source, other], passed.at[kind, source]
        ).wait()
        live = jnp.where(kind == 0, (z >= 1).astype(jnp.int32), ((source < me) | (z >= 2)).astype(jnp.int32))

        @pl.when(live == 1)
        def _():
            attend(kv.at[kind, source, 0], kv.at[kind, source, 1], False)

        return carry

    lax.fori_loop(0, 2 * PLANE, visit, 0)

    for head in range(HEADS):
        total = jnp.sum(run_sum[head], axis=0, keepdims=True)
        done = (run_out[head] / total).astype(jnp.bfloat16)
        for part in range(2):
            turned_out[part, 64 * head : 64 * head + 64, :] = done[:, HALF * part : HALF * part + HALF]
    heads_copy = remote(
        turned_out.at[other], heads_buf.at[tp], heads_send, heads_got, (sp, other)
    )
    heads_copy.start()
    heads_buf[tp] = turned_out[tp]
    local_copies[0].wait()
    heads_copy.wait_recv()

    attended = jnp.concatenate(
        [heads_buf[g].astype(jnp.float32).T.astype(jnp.bfloat16) for g in range(2)], axis=1
    )
    squares = jnp.zeros((HALF, 1), jnp.float32)
    for n in range(4):
        cols = slice(512 * n, 512 * n + 512)
        part = nn(attended, proj[:, cols])
        mix[:, cols] = part
        squares = squares + jnp.sum(part * part, axis=1, keepdims=True)
    scale = lax.rsqrt(squares * (1.0 / D) + epsilon)
    squares = jnp.zeros((HALF, 1), jnp.float32)
    for n in range(4):
        cols = slice(512 * n, 512 * n + 512)
        branch = mix[:, cols] * scale * mix_gain_ref[:, cols]
        mid = (residual_ref[:, cols].astype(jnp.float32) + branch).astype(jnp.bfloat16)
        middle[:, cols] = mid
        wide = mid.astype(jnp.float32)
        squares = squares + jnp.sum(wide * wide, axis=1, keepdims=True)
    scale = lax.rsqrt(squares * (1.0 / D) + epsilon)
    for n in range(4):
        cols = slice(512 * n, 512 * n + 512)
        normed[:, cols] = (
            middle[:, cols].astype(jnp.float32) * scale * moe_gain_ref[:, cols]
        ).astype(jnp.bfloat16)

    at_row = lax.broadcasted_iota(jnp.int32, (HALF, HALF), 0)
    at_col = lax.broadcasted_iota(jnp.int32, (HALF, HALF), 1)
    expert_row = lax.broadcasted_iota(jnp.int32, (EXPERTS, HALF), 0)
    hot = [(expert_row == ids_t_ref[k : k + 1, :]).astype(jnp.float32) for k in range(2)]
    earlier = nn(
        (hot[0] + hot[1]).astype(jnp.bfloat16), (at_row < at_col).astype(jnp.float32).astype(jnp.bfloat16)
    )
    slot_row = lax.broadcasted_iota(jnp.int32, (EXPERTS * CAP, HALF), 0)
    chooser = jnp.zeros((EXPERTS * CAP, HALF), jnp.float32)
    for k in range(2):
        rank = jnp.sum(hot[k] * earlier, axis=0, keepdims=True).astype(jnp.int32)
        slot = ids_t_ref[k : k + 1, :] * CAP + rank
        chooser = chooser + (slot_row == slot).astype(jnp.float32)
    chooser = chooser.astype(jnp.bfloat16)
    for n in range(8):
        cols = slice(256 * n, 256 * n + 256)
        picked = nn(chooser, normed[:, cols]).astype(jnp.bfloat16)
        send_buf[:, :, cols] = picked.reshape(EXPERTS, CAP, 256)

    def go_copy(step):
        target = (sp + step) % EXPERTS
        return remote(
            send_buf.at[target], recv_buf.at[sp], go_send.at[step], go_got.at[sp], (target, tp)
        )

    def go(step, carry):
        go_copy(step).start()
        return carry

    lax.fori_loop(1, EXPERTS, go, 0)
    mine = pltpu.make_async_copy(send_buf.at[sp], recv_buf.at[sp], own_copy)
    mine.start()
    for copy in local_copies[1:]:
        copy.wait()
    for copy in weight_copies:
        copy.wait_recv()
    mine.wait()

    def back_copy(source):
        return remote(
            done_buf.at[source], back_buf.at[sp], back_send.at[source], back_got.at[sp], (source, tp)
        )

    def expert_group(number, carry):
        group = (z - number + DEPTH) % DEPTH
        first = group * PLANE

        def await_rows(i, c):
            source = first + i

            @pl.when(source != sp)
            def _():
                pltpu.make_async_copy(
                    recv_buf.at[source], recv_buf.at[source], go_got.at[source]
                ).wait()

            return c

        lax.fori_loop(0, PLANE, await_rows, 0)
        rows = recv_buf[pl.ds(first, PLANE)].reshape(PLANE * CAP, D)
        hidden = []
        for half in range(2):
            gate_out = nn(rows, gate_w[half])
            up_out = nn(rows, up_w[half])
            hidden.append((gate_out / (1.0 + jnp.exp(-gate_out)) * up_out).astype(jnp.bfloat16))
        for n in range(4):
            cols = slice(512 * n, 512 * n + 512)
            parts = [
                nn(hidden[half], down_w[half, :, cols]).astype(jnp.bfloat16).astype(jnp.float32)
                for half in range(2)
            ]
            done_buf[pl.ds(first, PLANE), :, cols] = (
                (parts[0] + parts[1]).astype(jnp.bfloat16).reshape(PLANE, CAP, 512)
            )

        def send_back(i, c):
            source = first + i

            @pl.when(source != sp)
            def _():
                back_copy(source).start()

            return c

        lax.fori_loop(0, PLANE, send_back, 0)
        return carry

    lax.fori_loop(0, DEPTH, expert_group, 0)
    mine_back = pltpu.make_async_copy(done_buf.at[sp], back_buf.at[sp], own_copy)
    mine_back.start()

    expert_col = lax.broadcasted_iota(jnp.int32, (HALF, EXPERTS), 1)
    hot = [(expert_col == ids_ref[:, k : k + 1]).astype(jnp.float32) for k in range(2)]
    earlier = nn(
        (at_col < at_row).astype(jnp.float32).astype(jnp.bfloat16), (hot[0] + hot[1]).astype(jnp.bfloat16)
    )
    slot_col = lax.broadcasted_iota(jnp.int32, (HALF, EXPERTS * CAP), 1)
    takers = []
    for k in range(2):
        rank = jnp.sum(hot[k] * earlier, axis=1, keepdims=True).astype(jnp.int32)
        slot = ids_ref[:, k : k + 1] * CAP + rank
        takers.append((slot_col == slot).astype(jnp.float32).astype(jnp.bfloat16))

    mine_back.wait()

    def await_back(step, carry):
        source = (sp + step) % EXPERTS
        pltpu.make_async_copy(
            back_buf.at[source], back_buf.at[source], back_got.at[source]
        ).wait()
        return carry

    lax.fori_loop(1, EXPERTS, await_back, 0)
    for n in range(4):
        cols = slice(512 * n, 512 * n + 512)
        came = back_buf[:, :, cols].reshape(EXPERTS * CAP, 512)
        both = (
            nn(takers[0], came) * route_ref[:, 0:1] + nn(takers[1], came) * route_ref[:, 1:2]
        )
        out_ref[:, cols] = (middle[:, cols].astype(jnp.float32) + both).astype(jnp.bfloat16)

    for copy in next_z:
        copy.wait_send()
    for copy in weight_copies:
        copy.wait_send()
    heads_copy.wait_send()

    def plane_done(step, carry):
        plane_copy(0, step, True).wait_send()
        plane_copy(1, step, True).wait_send()
        return carry

    lax.fori_loop(1, PLANE, plane_done, 0)

    def pass_done(source, carry):
        pass_copy(0, source).wait_send()
        pass_copy(1, source).wait_send()
        return carry

    lax.fori_loop(0, PLANE, pass_done, 0)

    def moe_done(step, carry):
        go_copy(step).wait_send()
        back_copy((sp + step) % EXPERTS).wait_send()
        return carry

    lax.fori_loop(1, EXPERTS, moe_done, 0)


def local(
    residual,
    queries,
    latent,
    rope_key,
    doc_ids,
    latent_to_key,
    latent_to_value,
    out_proj,
    mix_gain,
    moe_gain,
    expert_ids,
    route_weight,
    gate_weight,
    up_weight,
    down_weight,
):
    bf16, f32 = jnp.bfloat16, jnp.float32
    first = lax.axis_index("sp") * ROWS
    positions = (first + jnp.arange(ROWS, dtype=jnp.int32)).astype(f32)
    half_width = ROPE // 2
    frequency = rope_base ** (-jnp.arange(half_width, dtype=f32) / half_width)
    angles = positions[:, None] * frequency[None, :]
    cosine, sine_part = jnp.cos(angles), jnp.sin(angles)
    hot = (doc_ids[:, None] == jnp.arange(8, dtype=jnp.int32)[None, :]).astype(f32)
    key_extra = jnp.concatenate(
        [rotate(rope_key, cosine, sine_part), hot.astype(bf16), jnp.zeros((ROWS, 24), bf16)], axis=1
    )
    key_extra = (
        key_extra.reshape(2, 4, 32, 64).transpose(0, 2, 1, 3).reshape(2, PIECE - HALF, LATENT)
    )
    own = jnp.concatenate([latent.reshape(2, HALF, LATENT), key_extra], axis=1)
    shaped = queries.reshape(ROWS, HEADS, UNROTATED_DIM + ROPE)
    plain = shaped[..., :UNROTATED_DIM]
    turned = rotate(shaped[..., UNROTATED_DIM:], cosine[:, None, :], sine_part[:, None, :])
    mask = jnp.broadcast_to(((hot - 1.0) * MASKED).astype(bf16)[:, None, :], (ROWS, HEADS, 8))
    extra = jnp.concatenate([turned, mask, jnp.zeros((ROWS, HEADS, 24), bf16)], axis=2)
    even = jnp.concatenate([plain[:, 0::2], extra[:, 0::2]], axis=2)
    odd = jnp.concatenate([extra[:, 1::2], plain[:, 1::2]], axis=2)
    query = jnp.stack([even, odd], axis=2).reshape(ROWS, HEADS, 128).transpose(1, 2, 0)

    vmem = pl.BlockSpec(memory_space=pltpu.VMEM)
    anywhere = pl.BlockSpec(memory_space=pl.ANY)
    dma = pltpu.SemaphoreType.DMA
    return pl.pallas_call(
        kernel,
        out_shape=jax.ShapeDtypeStruct((HALF, D), bf16),
        in_specs=[vmem] * 10 + [anywhere] * 4,
        out_specs=vmem,
        scratch_shapes=[
            pltpu.VMEM((2, PLANE, 2, PIECE, LATENT), bf16),
            pltpu.VMEM((HEADS, 1, ROWS), f32),
            pltpu.VMEM((HEADS, 8, ROWS), f32),
            pltpu.VMEM((HEADS, 64, ROWS), f32),
            pltpu.VMEM((2, HEADS * 64, HALF), bf16),
            pltpu.VMEM((2, HEADS * 64, HALF), bf16),
            pltpu.VMEM((2 * HEADS * 64, D), bf16),
            pltpu.VMEM((2, D, FF_HALF), bf16),
            pltpu.VMEM((2, D, FF_HALF), bf16),
            pltpu.VMEM((2, FF_HALF, D), bf16),
            pltpu.VMEM((HALF, D), f32),
            pltpu.VMEM((HALF, D), bf16),
            pltpu.VMEM((HALF, D), bf16),
            pltpu.VMEM((EXPERTS, CAP, D), bf16),
            pltpu.VMEM((EXPERTS, CAP, D), bf16),
            pltpu.VMEM((EXPERTS, CAP, D), bf16),
            pltpu.VMEM((EXPERTS, CAP, D), bf16),
            dma((2,)),
            dma((2, PLANE)),
            dma((2, PLANE)),
            dma((2, PLANE)),
            dma((2, PLANE)),
            dma((4,)),
            dma((3,)),
            dma((3,)),
            dma,
            dma,
            dma((EXPERTS,)),
            dma((EXPERTS,)),
            dma,
            dma((EXPERTS,)),
            dma((EXPERTS,)),
        ],
        compiler_params=pltpu.CompilerParams(
            collective_id=0, has_side_effects=True, vmem_limit_bytes=60 * 1024 * 1024
        ),
    )(
        query,
        own,
        latent_to_key,
        latent_to_value.T,
        residual,
        mix_gain.reshape(1, D),
        moe_gain.reshape(1, D),
        expert_ids,
        expert_ids.T,
        route_weight,
        out_proj,
        gate_weight,
        up_weight,
        down_weight,
    )


def solution(mesh):
    in_specs = (
        P(("sp", "tp"), None),
        P("sp", "tp"),
        P("sp", None),
        P("sp", None),
        P("sp"),
        P(None, "tp"),
        P(None, "tp"),
        P(),
        P(),
        P(),
        P(("sp", "tp"), None),
        P(("sp", "tp"), None),
        P("sp", None, "tp"),
        P("sp", None, "tp"),
        P("sp", "tp", None),
    )
    out_specs = P(("sp", "tp"), None)
    return jax.shard_map(local, mesh=mesh, in_specs=in_specs, out_specs=out_specs, check_vma=False)
```

```python
import functools

import jax
import jax.numpy as jnp
from jax import lax
from jax.experimental import pallas as pl
from jax.experimental.pallas import tpu as pltpu
from jax.sharding import PartitionSpec as P

D = 2048
UNROTATED_DIM = 64
ROPE = 32
HEADS = 6
LATENT = 256
ROWS = 256
HALF = 128
PIECE = 160
EXPERTS = 64
CAP = 8
FF_HALF = 512
PLANE = 16
DEPTH = 4
GROUP = 2
GROUPS = HEADS // GROUP
CHUNK = 64
STEP = 4 * ROWS
DEAD = 40
rope_base = 10000.0
epsilon = 1e-06
MASKED = 1e30
SCORE_BASE2 = float((UNROTATED_DIM + ROPE) ** (-0.5) * 1.4426950408889634)
MESH = pl.DeviceIdType.MESH


def hops(offset):
    return [min(v, DEPTH - v) for v in offset]


def exchange_order():
    cube = [(a, b, c) for a in range(DEPTH) for b in range(DEPTH) for c in range(DEPTH)]
    classes = []
    for kind in range(DEPTH):
        left = [o for o in cube if sum(o) % DEPTH == kind and any(o)]
        order, load = [], [0, 0, 0]
        while left:
            best = min(
                left,
                key=lambda o: (
                    max(a + b for a, b in zip(load, hops(o))) - min(a + b for a, b in zip(load, hops(o))),
                    -sum(hops(o)),
                    o,
                ),
            )
            left.remove(best)
            order.append(best)
            load = [a + b for a, b in zip(load, hops(best))]
        classes.append(order if kind else order + [(0, 0, 0)])
    return classes


ORDER = exchange_order()
OWN_SLOT = PLANE - 1


def rotate(source, cosine, sine_part):
    half_width = source.shape[-1] // 2
    upper_half = source[..., :half_width].astype(jnp.float32)
    lower_half = source[..., half_width:].astype(jnp.float32)
    turned = jnp.concatenate(
        [
            upper_half * cosine - lower_half * sine_part,
            lower_half * cosine + upper_half * sine_part,
        ],
        axis=-1,
    )
    return turned.astype(jnp.bfloat16)


def nn(a, b):
    return lax.dot_general(a, b, (((1,), (0,)), ((), ())), preferred_element_type=jnp.float32)


def nt(a, b):
    return lax.dot_general(a, b, (((1,), (1,)), ((), ())), preferred_element_type=jnp.float32)


def kernel(
    query_ref,
    own_ref,
    key_w_ref,
    value_w_ref,
    residual_ref,
    mix_gain_ref,
    moe_gain_ref,
    ids_ref,
    ids_t_ref,
    route_ref,
    proj_hbm,
    gate_hbm,
    up_hbm,
    down_hbm,
    out_ref,
    kv,
    run_max,
    held,
    tops,
    factors,
    probs,
    full_keys,
    values,
    run_out,
    turned_out,
    heads_buf,
    proj,
    gate_w,
    up_w,
    down_w,
    mix,
    middle,
    normed,
    send_buf,
    recv_buf,
    done_buf,
    back_buf,
    z_send,
    plane_send,
    pass_send,
    got,
    passed,
    weight_local,
    weight_send,
    weight_got,
    heads_send,
    heads_got,
    go_send,
    go_got,
    own_copy,
    back_send,
    back_got,
):
    sp = lax.axis_index("sp")
    tp = lax.axis_index("tp")
    other = 1 - tp
    z = sp // PLANE
    me = sp % PLANE

    def remote(src, dst, send_sem, recv_sem, device):
        return pltpu.make_async_remote_copy(
            src_ref=src,
            dst_ref=dst,
            send_sem=send_sem,
            recv_sem=recv_sem,
            device_id=device,
            device_id_type=MESH,
        )

    barrier = pltpu.get_barrier_semaphore()
    pl.semaphore_signal(barrier, inc=1, device_id=(sp, other), device_id_type=MESH)

    def greet(step, carry):
        pl.semaphore_signal(
            barrier, inc=1, device_id=((sp + step) % EXPERTS, tp), device_id_type=MESH
        )
        return carry

    lax.fori_loop(1, EXPERTS, greet, 0)

    local_copies = [
        pltpu.make_async_copy(proj_hbm, proj, weight_local.at[0]),
        pltpu.make_async_copy(gate_hbm.at[0], gate_w.at[tp], weight_local.at[1]),
        pltpu.make_async_copy(up_hbm.at[0], up_w.at[tp], weight_local.at[2]),
        pltpu.make_async_copy(down_hbm.at[0], down_w.at[tp], weight_local.at[3]),
    ]
    for copy in local_copies:
        copy.start()

    pl.semaphore_wait(barrier, EXPERTS)

    next_z = []
    for hop in (1, 2):
        target = ((z + hop) % DEPTH) * PLANE + me
        copy = remote(
            own_ref.at[tp],
            kv.at[hop - 1, me, tp],
            z_send.at[hop - 1],
            got.at[hop - 1, me],
            (target, tp),
        )
        copy.start()
        next_z.append(copy)

    def plane_copy(kind, step, own):
        peer = (me + step) % PLANE
        return remote(
            own_ref.at[tp] if own else kv.at[kind, me, tp],
            kv.at[kind, me, tp],
            plane_send.at[kind, step],
            got.at[kind, me],
            (z * PLANE + peer, tp),
        )

    def send_own(step, carry):
        @pl.when((me + step) % PLANE > me)
        def _():
            plane_copy(1, step, True).start()

        return carry

    lax.fori_loop(1, PLANE, send_own, 0)

    weight_copies = [
        remote(src.at[0], dst.at[tp], weight_send.at[i], weight_got.at[i], (sp, other))
        for i, (src, dst) in enumerate(((gate_hbm, gate_w), (up_hbm, up_w), (down_hbm, down_w)))
    ]
    for copy in weight_copies:
        copy.start()

    values[...] = jnp.ones_like(values)
    low_lanes = lax.broadcasted_iota(jnp.int32, (HALF, 128), 1) < 64
    dead_lane = (lax.broadcasted_iota(jnp.int32, (PIECE - HALF, 128), 1) % 64 == DEAD).astype(
        jnp.float32
    )

    def project(blocks, dead, bank):
        for number, (block, flag) in enumerate(zip(blocks, dead)):
            at = ROWS * number
            for half in range(2):
                low, high = [], []
                for tile in range(2):
                    extra = block[half, HALF:PIECE, 128 * tile : 128 * tile + 128].astype(jnp.float32)
                    if flag is not None:
                        extra = extra + dead_lane * flag
                    swapped = pltpu.roll(extra, 64, 1)
                    low += [extra, swapped]
                    high += [swapped, extra]
                low = jnp.concatenate(low, axis=0).astype(jnp.bfloat16)
                high = jnp.concatenate(high, axis=0).astype(jnp.bfloat16)
                keys = nn(block[half, :HALF, :], key_w_ref[...]).astype(jnp.bfloat16)
                for head in range(HEADS):
                    column = keys[:, 128 * (head // 2) : 128 * (head // 2) + 128]
                    if head % 2 == 0:
                        full_key = jnp.where(low_lanes, column, high)
                    else:
                        full_key = jnp.where(low_lanes, low, column)
                    full_keys[head, at + HALF * half : at + HALF * half + HALF, :] = full_key
            rows = jnp.concatenate([block[0, :HALF, :], block[1, :HALF, :]], axis=0)
            every = nt(value_w_ref[...], rows).astype(jnp.bfloat16)
            for head in range(HEADS):
                values[bank, head, :64, at : at + ROWS] = every[64 * head : 64 * head + 64, :]

    def score(first, slot, keys_at, causal):
        for i in range(GROUP):
            head = first + i
            top = None
            for number in range(keys_at // HALF):
                at = HALF * number
                scores = nn(full_keys[head, at : at + HALF, :], query_ref[head])
                if causal:
                    key_at = lax.broadcasted_iota(jnp.int32, (HALF, ROWS), 0) + at
                    query_at = lax.broadcasted_iota(jnp.int32, (HALF, ROWS), 1)
                    scores = jnp.where(key_at <= query_at, scores, -MASKED)
                held[slot, i, at : at + HALF, :] = scores
                here = jnp.max(scores.reshape(HALF // 8, 8, ROWS), axis=0)
                top = here if top is None else jnp.maximum(top, here)
            tops[slot, i] = jnp.max(top, axis=0, keepdims=True)

    def weigh(first, slot, keys_at, causal):
        for i in range(GROUP):
            head = first + i
            if causal:
                new_max = tops[slot, i]
            else:
                old_max = run_max[head]
                new_max = jnp.maximum(old_max, tops[slot, i])
                factors[head] = jnp.exp2((old_max - new_max) * SCORE_BASE2)
            run_max[head] = new_max
            for number in range(keys_at // CHUNK):
                at = CHUNK * number
                probs[slot, i, at : at + CHUNK, :] = jnp.exp2(
                    (held[slot, i, at : at + CHUNK, :] - new_max) * SCORE_BASE2
                ).astype(jnp.bfloat16)

    def gather_values(first, slot, keys_at, bank, causal):
        for i in range(GROUP):
            head = first + i
            part = nn(values[bank, head, :, :keys_at], probs[slot, i, :keys_at, :])
            if causal:
                run_out[head] = part
            else:
                run_out[head] = run_out[head] * factors[head] + part

    project([own_ref], [None], 1)
    for j in range(GROUPS):
        score(j * GROUP, j % 2, ROWS, True)
        weigh(j * GROUP, j % 2, ROWS, True)
        gather_values(j * GROUP, j % 2, ROWS, 1, True)

    def pass_copy(kind, source):
        return remote(
            kv.at[kind, source, tp],
            kv.at[kind, source, tp],
            pass_send.at[kind, source],
            passed.at[kind, source],
            (sp, other),
        )

    def arrival(kind, source):
        return pltpu.make_async_copy(
            kv.at[kind, source, tp], kv.at[kind, source, tp], got.at[kind, source]
        )

    arrival(0, me).wait()
    pass_copy(0, me).start()

    def send_first(step, carry):
        plane_copy(0, step, False).start()
        return carry

    lax.fori_loop(1, PLANE, send_first, 0)
    arrival(1, me).wait()
    pass_copy(1, me).start()

    def send_second(step, carry):
        @pl.when((me + step) % PLANE < me)
        def _():
            plane_copy(1, step, False).start()

        return carry

    lax.fori_loop(1, PLANE, send_second, 0)
    before = (me - 1 + PLANE) % PLANE
    for kind in range(2):
        arrival(kind, before).wait()
        pass_copy(kind, before).start()

    steps = jnp.where(z >= 1, PLANE // 2, me // 2 + 1)
    last_slot = (GROUPS - 1) % 2
    last_head = (GROUPS - 1) * GROUP

    def visit(step, carry):
        sources = [(me - 2 * step - i + PLANE) % PLANE for i in range(2)]

        @pl.when(step < PLANE // 2 - 1)
        def _():
            for i in range(2):
                later = (me - 2 * step - 2 - i + PLANE) % PLANE
                for kind in range(2):
                    arrival(kind, later).wait()
                    pass_copy(kind, later).start()

        for source in sources:
            for kind in range(2):
                pltpu.make_async_copy(
                    kv.at[kind, source, other], kv.at[kind, source, other], passed.at[kind, source]
                ).wait()

        @pl.when(step < steps)
        def _():
            bank = step % 2
            blocks, dead = [], []
            for source in sources:
                blocks += [kv.at[0, source], kv.at[1, source]]
                dead += [
                    (z < 1).astype(jnp.float32),
                    ((source >= me) & (z < 2)).astype(jnp.float32),
                ]

            project(blocks, dead, bank)
            score(0, 0, STEP, False)

            for j in range(GROUPS - 1):

                @pl.when(step >= -1 - j)
                def _(j=j):
                    if j > 0:
                        gather_values((j - 1) * GROUP, (j - 1) % 2, STEP, bank, False)
                    weigh(j * GROUP, j % 2, STEP, False)
                    score((j + 1) * GROUP, (j + 1) % 2, STEP, False)

            gather_values(last_head - GROUP, (last_slot + 1) % 2, STEP, bank, False)
            weigh(last_head, last_slot, STEP, False)
            gather_values(last_head, last_slot, STEP, bank, False)

        return carry

    lax.fori_loop(0, PLANE // 2, visit, 0)

    for head in range(HEADS):
        done = (run_out[head, :64, :] / run_out[head, 64:65, :]).astype(jnp.bfloat16)
        for part in range(2):
            turned_out[part, 64 * head : 64 * head + 64, :] = done[:, HALF * part : HALF * part + HALF]
    heads_copy = remote(
        turned_out.at[other], heads_buf.at[tp], heads_send, heads_got, (sp, other)
    )
    heads_copy.start()
    heads_buf[tp] = turned_out[tp]
    local_copies[0].wait()
    heads_copy.wait_recv()

    attended = jnp.concatenate(
        [heads_buf[g].astype(jnp.float32).T.astype(jnp.bfloat16) for g in range(2)], axis=1
    )
    squares = jnp.zeros((HALF, 1), jnp.float32)
    for n in range(4):
        cols = slice(512 * n, 512 * n + 512)
        part = nn(attended, proj[:, cols])
        mix[:, cols] = part
        squares = squares + jnp.sum(part * part, axis=1, keepdims=True)
    scale = lax.rsqrt(squares * (1.0 / D) + epsilon)
    squares = jnp.zeros((HALF, 1), jnp.float32)
    for n in range(4):
        cols = slice(512 * n, 512 * n + 512)
        branch = mix[:, cols] * scale * mix_gain_ref[:, cols]
        mid = (residual_ref[:, cols].astype(jnp.float32) + branch).astype(jnp.bfloat16)
        middle[:, cols] = mid
        wide = mid.astype(jnp.float32)
        squares = squares + jnp.sum(wide * wide, axis=1, keepdims=True)
    scale = lax.rsqrt(squares * (1.0 / D) + epsilon)
    for n in range(4):
        cols = slice(512 * n, 512 * n + 512)
        normed[:, cols] = (
            middle[:, cols].astype(jnp.float32) * scale * moe_gain_ref[:, cols]
        ).astype(jnp.bfloat16)

    at_row = lax.broadcasted_iota(jnp.int32, (HALF, HALF), 0)
    at_col = lax.broadcasted_iota(jnp.int32, (HALF, HALF), 1)
    expert_row = lax.broadcasted_iota(jnp.int32, (EXPERTS, HALF), 0)
    hot = [(expert_row == ids_t_ref[k : k + 1, :]).astype(jnp.float32) for k in range(2)]
    earlier = nn(
        (hot[0] + hot[1]).astype(jnp.bfloat16), (at_row < at_col).astype(jnp.float32).astype(jnp.bfloat16)
    )
    slot_row = lax.broadcasted_iota(jnp.int32, (EXPERTS * CAP, HALF), 0)
    chooser = jnp.zeros((EXPERTS * CAP, HALF), jnp.float32)
    for k in range(2):
        rank = jnp.sum(hot[k] * earlier, axis=0, keepdims=True).astype(jnp.int32)
        slot = ids_t_ref[k : k + 1, :] * CAP + rank
        chooser = chooser + (slot_row == slot).astype(jnp.float32)
    chooser = chooser.astype(jnp.bfloat16)
    for n in range(8):
        cols = slice(256 * n, 256 * n + 256)
        picked = nn(chooser, normed[:, cols]).astype(jnp.bfloat16)
        send_buf[:, :, cols] = picked.reshape(EXPERTS, CAP, 256)

    y, x = me // DEPTH, me % DEPTH

    def toward(offset, sign):
        dz, dy, dx = offset
        return (
            ((z + sign * dz + DEPTH) % DEPTH) * PLANE
            + ((y + sign * dy + DEPTH) % DEPTH) * DEPTH
            + (x + sign * dx + DEPTH) % DEPTH
        )

    def go_copy(kind, i):
        target = toward(ORDER[kind][i], 1)
        slot = kind * PLANE + i
        return remote(
            send_buf.at[target], recv_buf.at[slot], go_send.at[slot], go_got.at[slot], (target, tp)
        )

    def back_copy(kind, i):
        source = toward(ORDER[kind][i], -1)
        slot = kind * PLANE + i
        return remote(
            done_buf.at[slot], back_buf.at[sp], back_send.at[slot], back_got.at[sp], (source, tp)
        )

    away = [(kind, i) for kind in range(DEPTH) for i in range(PLANE) if any(ORDER[kind][i])]
    for kind, i in away:
        go_copy(kind, i).start()
    mine = pltpu.make_async_copy(send_buf.at[sp], recv_buf.at[OWN_SLOT], own_copy)
    mine.start()
    for copy in local_copies[1:]:
        copy.wait()
    for copy in weight_copies:
        copy.wait_recv()
    mine.wait()

    def expert_group(kind, carry):
        first = kind * PLANE
        rows = recv_buf[pl.ds(first, PLANE)].reshape(PLANE * CAP, D)
        hidden = []
        for half in range(2):
            gate_out = nn(rows, gate_w[half])
            up_out = nn(rows, up_w[half])
            hidden.append((gate_out / (1.0 + jnp.exp(-gate_out)) * up_out).astype(jnp.bfloat16))
        for n in range(4):
            cols = slice(512 * n, 512 * n + 512)
            parts = [
                nn(hidden[half], down_w[half, :, cols]).astype(jnp.bfloat16).astype(jnp.float32)
                for half in range(2)
            ]
            done_buf[pl.ds(first, PLANE), :, cols] = (
                (parts[0] + parts[1]).astype(jnp.bfloat16).reshape(PLANE, CAP, 512)
            )

    def turn(kind, carry):
        for k in range(DEPTH):

            @pl.when(kind == k)
            def _(k=k):
                for i in range(PLANE):
                    if any(ORDER[k][i]):
                        slot = k * PLANE + i
                        pltpu.make_async_copy(
                            recv_buf.at[slot], recv_buf.at[slot], go_got.at[slot]
                        ).wait()

        expert_group(kind, carry)
        for k in range(DEPTH):

            @pl.when(kind == k)
            def _(k=k):
                for i in range(PLANE):
                    if any(ORDER[k][i]):
                        back_copy(k, i).start()

        return carry

    lax.fori_loop(0, DEPTH, turn, 0)
    mine_back = pltpu.make_async_copy(done_buf.at[OWN_SLOT], back_buf.at[sp], own_copy)
    mine_back.start()

    expert_col = lax.broadcasted_iota(jnp.int32, (HALF, EXPERTS), 1)
    hot = [(expert_col == ids_ref[:, k : k + 1]).astype(jnp.float32) for k in range(2)]
    earlier = nn(
        (at_col < at_row).astype(jnp.float32).astype(jnp.bfloat16), (hot[0] + hot[1]).astype(jnp.bfloat16)
    )
    slot_col = lax.broadcasted_iota(jnp.int32, (HALF, EXPERTS * CAP), 1)
    takers = []
    for k in range(2):
        rank = jnp.sum(hot[k] * earlier, axis=1, keepdims=True).astype(jnp.int32)
        slot = ids_ref[:, k : k + 1] * CAP + rank
        takers.append((slot_col == slot).astype(jnp.float32).astype(jnp.bfloat16))

    mine_back.wait()

    def await_back(step, carry):
        source = (sp + step) % EXPERTS
        pltpu.make_async_copy(
            back_buf.at[source], back_buf.at[source], back_got.at[source]
        ).wait()
        return carry

    lax.fori_loop(1, EXPERTS, await_back, 0)
    for n in range(4):
        cols = slice(512 * n, 512 * n + 512)
        came = back_buf[:, :, cols].reshape(EXPERTS * CAP, 512)
        both = (
            nn(takers[0], came) * route_ref[:, 0:1] + nn(takers[1], came) * route_ref[:, 1:2]
        )
        out_ref[:, cols] = (middle[:, cols].astype(jnp.float32) + both).astype(jnp.bfloat16)

    for copy in next_z:
        copy.wait_send()
    for copy in weight_copies:
        copy.wait_send()
    heads_copy.wait_send()

    def plane_done(step, carry):
        plane_copy(0, step, True).wait_send()
        plane_copy(1, step, True).wait_send()
        return carry

    lax.fori_loop(1, PLANE, plane_done, 0)

    def pass_done(source, carry):
        pass_copy(0, source).wait_send()
        pass_copy(1, source).wait_send()
        return carry

    lax.fori_loop(0, PLANE, pass_done, 0)

    for kind, i in away:
        go_copy(kind, i).wait_send()
        back_copy(kind, i).wait_send()


def local(
    residual,
    queries,
    latent,
    rope_key,
    doc_ids,
    latent_to_key,
    latent_to_value,
    out_proj,
    mix_gain,
    moe_gain,
    expert_ids,
    route_weight,
    gate_weight,
    up_weight,
    down_weight,
):
    bf16, f32 = jnp.bfloat16, jnp.float32
    first = lax.axis_index("sp") * ROWS
    positions = (first + jnp.arange(ROWS, dtype=jnp.int32)).astype(f32)
    half_width = ROPE // 2
    frequency = rope_base ** (-jnp.arange(half_width, dtype=f32) / half_width)
    angles = positions[:, None] * frequency[None, :]
    cosine, sine_part = jnp.cos(angles), jnp.sin(angles)
    hot = (doc_ids[:, None] == jnp.arange(8, dtype=jnp.int32)[None, :]).astype(f32)
    key_extra = jnp.concatenate(
        [rotate(rope_key, cosine, sine_part), hot.astype(bf16), jnp.zeros((ROWS, 24), bf16)], axis=1
    )
    key_extra = (
        key_extra.reshape(2, 4, 32, 64).transpose(0, 2, 1, 3).reshape(2, PIECE - HALF, LATENT)
    )
    own = jnp.concatenate([latent.reshape(2, HALF, LATENT), key_extra], axis=1)
    shaped = queries.reshape(ROWS, HEADS, UNROTATED_DIM + ROPE)
    plain = shaped[..., :UNROTATED_DIM]
    turned = rotate(shaped[..., UNROTATED_DIM:], cosine[:, None, :], sine_part[:, None, :])
    mask = jnp.broadcast_to(((hot - 1.0) * MASKED).astype(bf16)[:, None, :], (ROWS, HEADS, 8))
    extra = jnp.concatenate([turned, mask, jnp.full((ROWS, HEADS, 1), -MASKED, bf16), jnp.zeros((ROWS, HEADS, 23), bf16)], axis=2)
    even = jnp.concatenate([plain[:, 0::2], extra[:, 0::2]], axis=2)
    odd = jnp.concatenate([extra[:, 1::2], plain[:, 1::2]], axis=2)
    query = jnp.stack([even, odd], axis=2).reshape(ROWS, HEADS, 128).transpose(1, 2, 0)

    vmem = pl.BlockSpec(memory_space=pltpu.VMEM)
    anywhere = pl.BlockSpec(memory_space=pl.ANY)
    dma = pltpu.SemaphoreType.DMA
    return pl.pallas_call(
        kernel,
        out_shape=jax.ShapeDtypeStruct((HALF, D), bf16),
        in_specs=[vmem] * 10 + [anywhere] * 4,
        out_specs=vmem,
        scratch_shapes=[
            pltpu.VMEM((2, PLANE, 2, PIECE, LATENT), bf16),
            pltpu.VMEM((HEADS, 1, ROWS), f32),
            pltpu.VMEM((2, GROUP, STEP, ROWS), f32),
            pltpu.VMEM((2, GROUP, 1, ROWS), f32),
            pltpu.VMEM((HEADS, 1, ROWS), f32),
            pltpu.VMEM((2, GROUP, STEP, ROWS), bf16),
            pltpu.VMEM((HEADS, STEP, 128), bf16),
            pltpu.VMEM((2, HEADS, 80, STEP), bf16),
            pltpu.VMEM((HEADS, 80, ROWS), f32),
            pltpu.VMEM((2, HEADS * 64, HALF), bf16),
            pltpu.VMEM((2, HEADS * 64, HALF), bf16),
            pltpu.VMEM((2 * HEADS * 64, D), bf16),
            pltpu.VMEM((2, D, FF_HALF), bf16),
            pltpu.VMEM((2, D, FF_HALF), bf16),
            pltpu.VMEM((2, FF_HALF, D), bf16),
            pltpu.VMEM((HALF, D), f32),
            pltpu.VMEM((HALF, D), bf16),
            pltpu.VMEM((HALF, D), bf16),
            pltpu.VMEM((EXPERTS, CAP, D), bf16),
            pltpu.VMEM((EXPERTS, CAP, D), bf16),
            pltpu.VMEM((EXPERTS, CAP, D), bf16),
            pltpu.VMEM((EXPERTS, CAP, D), bf16),
            dma((2,)),
            dma((2, PLANE)),
            dma((2, PLANE)),
            dma((2, PLANE)),
            dma((2, PLANE)),
            dma((4,)),
            dma((3,)),
            dma((3,)),
            dma,
            dma,
            dma((EXPERTS,)),
            dma((EXPERTS,)),
            dma,
            dma((EXPERTS,)),
            dma((EXPERTS,)),
        ],
        compiler_params=pltpu.CompilerParams(
            collective_id=0, has_side_effects=True, vmem_limit_bytes=60 * 1024 * 1024
        ),
    )(
        query,
        own,
        latent_to_key,
        latent_to_value.T,
        residual,
        mix_gain.reshape(1, D),
        moe_gain.reshape(1, D),
        expert_ids,
        expert_ids.T,
        route_weight,
        out_proj,
        gate_weight,
        up_weight,
        down_weight,
    )


def solution(mesh):
    in_specs = (
        P(("sp", "tp"), None),
        P("sp", "tp"),
        P("sp", None),
        P("sp", None),
        P("sp"),
        P(None, "tp"),
        P(None, "tp"),
        P(),
        P(),
        P(),
        P(("sp", "tp"), None),
        P(("sp", "tp"), None),
        P("sp", None, "tp"),
        P("sp", None, "tp"),
        P("sp", "tp", None),
    )
    out_specs = P(("sp", "tp"), None)
    return jax.shard_map(local, mesh=mesh, in_specs=in_specs, out_specs=out_specs, check_vma=False)
```

```python
import functools

import jax
import jax.numpy as jnp
from jax import lax
from jax.experimental import pallas as pl
from jax.experimental.pallas import tpu as pltpu
from jax.sharding import PartitionSpec as P

D = 2048
UNROTATED_DIM = 64
ROPE = 32
HEADS = 6
LATENT = 256
ROWS = 256
HALF = 128
PIECE = 160
EXPERTS = 64
CAP = 8
FF_HALF = 512
PLANE = 16
DEPTH = 4
GROUP = 2
GROUPS = HEADS // GROUP
CHUNK = 64
STEP = 4 * ROWS
DEAD = 40
rope_base = 10000.0
epsilon = 1e-06
MASKED = 1e30
SCORE_BASE2 = float((UNROTATED_DIM + ROPE) ** (-0.5) * 1.4426950408889634)
MESH = pl.DeviceIdType.MESH


def hops(offset):
    return [min(v, DEPTH - v) for v in offset]


def exchange_order():
    cube = [(a, b, c) for a in range(DEPTH) for b in range(DEPTH) for c in range(DEPTH)]
    classes = []
    for kind in range(DEPTH):
        left = [o for o in cube if sum(o) % DEPTH == kind and any(o)]
        order, load = [], [0, 0, 0]
        while left:
            best = min(
                left,
                key=lambda o: (
                    max(a + b for a, b in zip(load, hops(o))) - min(a + b for a, b in zip(load, hops(o))),
                    -sum(hops(o)),
                    o,
                ),
            )
            left.remove(best)
            order.append(best)
            load = [a + b for a, b in zip(load, hops(best))]
        classes.append(order if kind else order + [(0, 0, 0)])
    return classes


ORDER = exchange_order()
OWN_SLOT = PLANE - 1
SEQUENCE = [(0, 0), (0, 1), (1, 0), (0, 3), (3, 0), (0, 2), (2, 0), (1, 1)]
SEQUENCE += [(1, 3), (3, 1), (3, 3), (1, 2), (2, 1), (3, 2), (2, 3), (2, 2)]


def turned(upper, lower, cosine, sine_part):
    return [upper * cosine - lower * sine_part, lower * cosine + upper * sine_part]


def nn(a, b):
    return lax.dot_general(a, b, (((1,), (0,)), ((), ())), preferred_element_type=jnp.float32)


def nt(a, b):
    return lax.dot_general(a, b, (((1,), (1,)), ((), ())), preferred_element_type=jnp.float32)


def kernel(
    raw_query_ref,
    latent_ref,
    rope_ref,
    doc_ref,
    cosine_ref,
    sine_ref,
    key_w_ref,
    raw_value_w_ref,
    residual_ref,
    mix_gain_ref,
    moe_gain_ref,
    ids_ref,
    route_ref,
    proj_hbm,
    gate_hbm,
    up_hbm,
    down_hbm,
    out_ref,
    own_ref,
    query_ref,
    value_w_ref,
    kv,
    run_max,
    held,
    tops,
    factors,
    probs,
    full_keys,
    values,
    run_out,
    turned_out,
    heads_buf,
    proj,
    gate_w,
    up_w,
    down_w,
    mix,
    middle,
    normed,
    send_buf,
    recv_buf,
    done_buf,
    back_buf,
    z_send,
    first_send,
    second_send,
    pass_send,
    got,
    passed,
    weight_local,
    weight_send,
    weight_got,
    heads_send,
    heads_got,
    go_send,
    go_got,
    own_copy,
    back_send,
    back_got,
):
    sp = lax.axis_index("sp")
    tp = lax.axis_index("tp")
    other = 1 - tp
    z = sp // PLANE
    me = sp % PLANE
    y, x = me // DEPTH, me % DEPTH

    def remote(src, dst, send_sem, recv_sem, device):
        return pltpu.make_async_remote_copy(
            src_ref=src,
            dst_ref=dst,
            send_sem=send_sem,
            recv_sem=recv_sem,
            device_id=device,
            device_id_type=MESH,
        )

    barrier = pltpu.get_barrier_semaphore()
    pl.semaphore_signal(barrier, inc=1, device_id=(sp, other), device_id_type=MESH)

    def greet(step, carry):
        pl.semaphore_signal(
            barrier, inc=1, device_id=((sp + step) % EXPERTS, tp), device_id_type=MESH
        )
        return carry

    lax.fori_loop(1, EXPERTS, greet, 0)

    local_copies = [
        pltpu.make_async_copy(proj_hbm, proj, weight_local.at[0]),
        pltpu.make_async_copy(gate_hbm.at[0], gate_w.at[tp], weight_local.at[1]),
        pltpu.make_async_copy(up_hbm.at[0], up_w.at[tp], weight_local.at[2]),
        pltpu.make_async_copy(down_hbm.at[0], down_w.at[tp], weight_local.at[3]),
    ]
    for copy in local_copies:
        copy.start()

    cosine, sine_part = cosine_ref[...], sine_ref[...]
    rope = rope_ref[...].astype(jnp.float32)
    hot = (lax.broadcasted_iota(jnp.int32, (8, ROWS), 0) == doc_ref[...]).astype(jnp.float32)
    extra = turned(rope[:16, :], rope[16:, :], cosine, sine_part) + [hot, jnp.zeros((24, ROWS), jnp.float32)]
    extra = jnp.concatenate(extra + extra, axis=0).T.astype(jnp.bfloat16)
    low_quarter = lax.broadcasted_iota(jnp.int32, (PIECE - HALF, 128), 1) < 64
    for half in range(2):
        own_ref[half, :HALF, :] = latent_ref[HALF * half : HALF * half + HALF, :]
        for tile in range(2):
            at = HALF * half + 64 * tile
            own_ref[half, HALF:PIECE, 128 * tile : 128 * tile + 128] = jnp.where(
                low_quarter, extra[at : at + 32, :], extra[at + 32 : at + 64, :]
            )
    keep = pltpu.make_async_copy(own_ref.at[tp], kv.at[2, me, tp], own_copy)
    keep.start()
    keep.wait()
    pl.semaphore_wait(barrier, EXPERTS)

    next_z = []
    for hop in (1, 2):
        target = ((z + hop) % DEPTH) * PLANE + me
        copy = remote(
            own_ref.at[tp],
            kv.at[hop - 1, me, tp],
            z_send.at[hop - 1],
            got.at[hop - 1, me],
            (target, tp),
        )
        copy.start()
        next_z.append(copy)

    def place(dy, dx):
        return ((y + dy + DEPTH) % DEPTH) * DEPTH + (x + dx + DEPTH) % DEPTH

    def first_peer(k):
        return jnp.where(tp == 0, place(k, 0), place(0, k))

    def second_peer(k):
        return jnp.where(tp == 0, place(0, k), place(k, 0))

    def first_copy(kind, k):
        peer = first_peer(k)
        later = peer > me
        source = (0, jnp.where(later, 2, 1), jnp.where(later, 1, 2))[kind]
        return remote(
            kv.at[source, me, tp],
            kv.at[kind, me, tp],
            first_send.at[kind, k],
            got.at[kind, me],
            (z * PLANE + peer, tp),
        )

    def second_copy(kind, k, j):
        peer = second_peer(k)
        later = peer > me
        origin = first_peer(-j)
        if kind == 0:
            source = 0
        elif j == 0:
            source = jnp.where(later, 2, 1)
        else:
            source = jnp.where((tp == 1) & ((origin < me) != later), 2, 1)
        return remote(
            kv.at[source, origin, tp],
            kv.at[kind, origin, tp],
            second_send.at[kind, k, j],
            got.at[kind, origin],
            (z * PLANE + peer, tp),
        )

    weight_copies = [
        remote(src.at[0], dst.at[tp], weight_send.at[i], weight_got.at[i], (sp, other))
        for i, (src, dst) in enumerate(((gate_hbm, gate_w), (up_hbm, up_w), (down_hbm, down_w)))
    ]
    for copy in weight_copies:
        copy.start()

    mask = (hot - 1.0) * MASKED
    dead_row = jnp.where(lax.broadcasted_iota(jnp.int32, (24, ROWS), 0) == 0, -MASKED, 0.0)
    flat = raw_query_ref[...].astype(jnp.float32)
    for head in range(HEADS):
        at = (UNROTATED_DIM + ROPE) * head
        plain = [flat[at : at + 64, :]]
        rest = turned(flat[at + 64 : at + 80, :], flat[at + 80 : at + 96, :], cosine, sine_part)
        rest = rest + [mask, dead_row]
        query_ref[head] = jnp.concatenate(
            plain + rest if head % 2 == 0 else rest + plain, axis=0
        ).astype(jnp.bfloat16)
    value_w_ref[...] = raw_value_w_ref[...].astype(jnp.float32).T.astype(jnp.bfloat16)
    values[...] = jnp.ones_like(values)
    low_lanes = lax.broadcasted_iota(jnp.int32, (HALF, 128), 1) < 64
    dead_lane = (lax.broadcasted_iota(jnp.int32, (PIECE - HALF, 128), 1) % 64 == DEAD).astype(
        jnp.float32
    )

    def project(blocks, dead, bank):
        for number, (block, flag) in enumerate(zip(blocks, dead)):
            at = ROWS * number
            for half in range(2):
                low, high = [], []
                for tile in range(2):
                    extra = block[half, HALF:PIECE, 128 * tile : 128 * tile + 128].astype(jnp.float32)
                    if flag is not None:
                        extra = extra + dead_lane * flag
                    swapped = pltpu.roll(extra, 64, 1)
                    low += [extra, swapped]
                    high += [swapped, extra]
                low = jnp.concatenate(low, axis=0).astype(jnp.bfloat16)
                high = jnp.concatenate(high, axis=0).astype(jnp.bfloat16)
                keys = nn(block[half, :HALF, :], key_w_ref[...]).astype(jnp.bfloat16)
                for head in range(HEADS):
                    column = keys[:, 128 * (head // 2) : 128 * (head // 2) + 128]
                    if head % 2 == 0:
                        full_key = jnp.where(low_lanes, column, high)
                    else:
                        full_key = jnp.where(low_lanes, low, column)
                    full_keys[head, at + HALF * half : at + HALF * half + HALF, :] = full_key
            rows = jnp.concatenate([block[0, :HALF, :], block[1, :HALF, :]], axis=0)
            every = nt(value_w_ref[...], rows).astype(jnp.bfloat16)
            for head in range(HEADS):
                values[bank, head, :64, at : at + ROWS] = every[64 * head : 64 * head + 64, :]

    def score(first, slot, keys_at, causal):
        for i in range(GROUP):
            head = first + i
            top = None
            for number in range(keys_at // HALF):
                at = HALF * number
                scores = nn(full_keys[head, at : at + HALF, :], query_ref[head])
                if causal:
                    key_at = lax.broadcasted_iota(jnp.int32, (HALF, ROWS), 0) + at
                    query_at = lax.broadcasted_iota(jnp.int32, (HALF, ROWS), 1)
                    scores = jnp.where(key_at <= query_at, scores, -MASKED)
                held[slot, i, at : at + HALF, :] = scores
                here = jnp.max(scores.reshape(HALF // 8, 8, ROWS), axis=0)
                top = here if top is None else jnp.maximum(top, here)
            tops[slot, i] = jnp.max(top, axis=0, keepdims=True)

    def weigh(first, slot, keys_at, causal):
        for i in range(GROUP):
            head = first + i
            if causal:
                new_max = tops[slot, i]
            else:
                old_max = run_max[head]
                new_max = jnp.maximum(old_max, tops[slot, i])
                factors[head] = jnp.exp2((old_max - new_max) * SCORE_BASE2)
            run_max[head] = new_max
            for number in range(keys_at // CHUNK):
                at = CHUNK * number
                probs[slot, i, at : at + CHUNK, :] = jnp.exp2(
                    (held[slot, i, at : at + CHUNK, :] - new_max) * SCORE_BASE2
                ).astype(jnp.bfloat16)

    def gather_values(first, slot, keys_at, bank, causal):
        for i in range(GROUP):
            head = first + i
            part = nn(values[bank, head, :, :keys_at], probs[slot, i, :keys_at, :])
            if causal:
                run_out[head] = part
            else:
                run_out[head] = run_out[head] * factors[head] + part

    project([own_ref], [None], 1)
    for j in range(GROUPS):
        score(j * GROUP, j % 2, ROWS, True)
        weigh(j * GROUP, j % 2, ROWS, True)
        gather_values(j * GROUP, j % 2, ROWS, 1, True)

    def pass_copy(kind, source):
        return remote(
            kv.at[kind, source, tp],
            kv.at[kind, source, tp],
            pass_send.at[kind, source],
            passed.at[kind, source],
            (sp, other),
        )

    def arrival(kind, source):
        return pltpu.make_async_copy(
            kv.at[kind, source, tp], kv.at[kind, source, tp], got.at[kind, source]
        )

    def take(origin):
        for kind in range(2):
            arrival(kind, origin).wait()
            pass_copy(kind, origin).start()

    def relay(j):
        origin = first_peer(-j)
        take(origin)

        @pl.when(tp == 1)
        def _():
            arrival(2, origin).wait()

        for k in (1, 3, 2):
            for kind in range(2):
                second_copy(kind, k, j).start()

    take(me)
    for k in (1, 3, 2):
        for kind in range(2):
            first_copy(kind, k).start()

        @pl.when(tp == 1)
        def _():
            first_copy(2, k).start()

        for kind in range(2):
            second_copy(kind, k, 0).start()
    for j in (1, 3):
        relay(j)
        take(second_peer(-j))

    last_slot = (GROUPS - 1) % 2
    last_head = (GROUPS - 1) * GROUP

    def visit(step, carry):
        @pl.when(step == 0)
        def _():
            relay(2)
            take(second_peer(-2))

        for n in range(1, len(SEQUENCE) // 2 - 1):
            ahead = [o for o in SEQUENCE[2 * n + 2 : 2 * n + 4] if o[0] and o[1]]
            if ahead:

                @pl.when(step == n)
                def _(ahead=ahead):
                    for dy, dx in ahead:
                        take(place(-dy, -dx))

        sources = []
        for i in range(2):
            dy, dx = 0, 0
            for n in range(len(SEQUENCE) // 2):
                dy = jnp.where(step == n, SEQUENCE[2 * n + i][0], dy)
                dx = jnp.where(step == n, SEQUENCE[2 * n + i][1], dx)
            sources.append(place(-dy, -dx))

        for source in sources:
            for kind in range(2):
                pltpu.make_async_copy(
                    kv.at[kind, source, other], kv.at[kind, source, other], passed.at[kind, source]
                ).wait()

        @pl.when(step >= 0)
        def _():
            bank = step % 2
            blocks, dead = [], []
            for source in sources:
                blocks += [kv.at[0, source], kv.at[1, source]]
                dead += [
                    (z < 1).astype(jnp.float32),
                    ((source >= me) & (z < 2)).astype(jnp.float32),
                ]

            project(blocks, dead, bank)
            score(0, 0, STEP, False)

            for j in range(GROUPS - 1):

                @pl.when(step >= -1 - j)
                def _(j=j):
                    if j > 0:
                        gather_values((j - 1) * GROUP, (j - 1) % 2, STEP, bank, False)
                    weigh(j * GROUP, j % 2, STEP, False)
                    score((j + 1) * GROUP, (j + 1) % 2, STEP, False)

            gather_values(last_head - GROUP, (last_slot + 1) % 2, STEP, bank, False)
            weigh(last_head, last_slot, STEP, False)
            gather_values(last_head, last_slot, STEP, bank, False)

        return carry

    lax.fori_loop(0, PLANE // 2, visit, 0)

    for head in range(HEADS):
        done = (run_out[head, :64, :] / run_out[head, 64:65, :]).astype(jnp.bfloat16)
        for part in range(2):
            turned_out[part, 64 * head : 64 * head + 64, :] = done[:, HALF * part : HALF * part + HALF]
    heads_copy = remote(
        turned_out.at[other], heads_buf.at[tp], heads_send, heads_got, (sp, other)
    )
    heads_copy.start()
    heads_buf[tp] = turned_out[tp]
    local_copies[0].wait()
    heads_copy.wait_recv()

    attended = jnp.concatenate(
        [heads_buf[g].astype(jnp.float32).T.astype(jnp.bfloat16) for g in range(2)], axis=1
    )
    squares = jnp.zeros((HALF, 1), jnp.float32)
    for n in range(4):
        cols = slice(512 * n, 512 * n + 512)
        part = nn(attended, proj[:, cols])
        mix[:, cols] = part
        squares = squares + jnp.sum(part * part, axis=1, keepdims=True)
    scale = lax.rsqrt(squares * (1.0 / D) + epsilon)
    squares = jnp.zeros((HALF, 1), jnp.float32)
    for n in range(4):
        cols = slice(512 * n, 512 * n + 512)
        branch = mix[:, cols] * scale * mix_gain_ref[:, cols]
        mid = (residual_ref[:, cols].astype(jnp.float32) + branch).astype(jnp.bfloat16)
        middle[:, cols] = mid
        wide = mid.astype(jnp.float32)
        squares = squares + jnp.sum(wide * wide, axis=1, keepdims=True)
    scale = lax.rsqrt(squares * (1.0 / D) + epsilon)
    for n in range(4):
        cols = slice(512 * n, 512 * n + 512)
        normed[:, cols] = (
            middle[:, cols].astype(jnp.float32) * scale * moe_gain_ref[:, cols]
        ).astype(jnp.bfloat16)

    at_row = lax.broadcasted_iota(jnp.int32, (HALF, HALF), 0)
    at_col = lax.broadcasted_iota(jnp.int32, (HALF, HALF), 1)
    expert_row = lax.broadcasted_iota(jnp.int32, (EXPERTS, HALF), 0)
    ids_t = ids_ref[...]
    hot = [(expert_row == ids_t[k : k + 1, :]).astype(jnp.float32) for k in range(2)]
    earlier = nn(
        (hot[0] + hot[1]).astype(jnp.bfloat16), (at_row < at_col).astype(jnp.float32).astype(jnp.bfloat16)
    )
    slot_row = lax.broadcasted_iota(jnp.int32, (EXPERTS * CAP, HALF), 0)
    chooser = jnp.zeros((EXPERTS * CAP, HALF), jnp.float32)
    for k in range(2):
        rank = jnp.sum(hot[k] * earlier, axis=0, keepdims=True).astype(jnp.int32)
        slot = ids_t[k : k + 1, :] * CAP + rank
        chooser = chooser + (slot_row == slot).astype(jnp.float32)
    chooser = chooser.astype(jnp.bfloat16)
    for n in range(8):
        cols = slice(256 * n, 256 * n + 256)
        picked = nn(chooser, normed[:, cols]).astype(jnp.bfloat16)
        send_buf[:, :, cols] = picked.reshape(EXPERTS, CAP, 256)

    def toward(offset, sign):
        dz, dy, dx = offset
        return (
            ((z + sign * dz + DEPTH) % DEPTH) * PLANE
            + ((y + sign * dy + DEPTH) % DEPTH) * DEPTH
            + (x + sign * dx + DEPTH) % DEPTH
        )

    def go_copy(kind, i):
        target = toward(ORDER[kind][i], 1)
        slot = kind * PLANE + i
        return remote(
            send_buf.at[target], recv_buf.at[slot], go_send.at[slot], go_got.at[slot], (target, tp)
        )

    def back_copy(kind, i):
        source = toward(ORDER[kind][i], -1)
        slot = kind * PLANE + i
        return remote(
            done_buf.at[slot], back_buf.at[sp], back_send.at[slot], back_got.at[sp], (source, tp)
        )

    away = [(kind, i) for kind in range(DEPTH) for i in range(PLANE) if any(ORDER[kind][i])]
    for kind, i in away:
        go_copy(kind, i).start()
    mine = pltpu.make_async_copy(send_buf.at[sp], recv_buf.at[OWN_SLOT], own_copy)
    mine.start()
    for copy in local_copies[1:]:
        copy.wait()
    for copy in weight_copies:
        copy.wait_recv()
    mine.wait()

    def expert_group(kind, carry):
        first = kind * PLANE
        rows = recv_buf[pl.ds(first, PLANE)].reshape(PLANE * CAP, D)
        hidden = []
        for half in range(2):
            gate_out = nn(rows, gate_w[half])
            up_out = nn(rows, up_w[half])
            hidden.append((gate_out / (1.0 + jnp.exp(-gate_out)) * up_out).astype(jnp.bfloat16))
        for n in range(4):
            cols = slice(512 * n, 512 * n + 512)
            parts = [
                nn(hidden[half], down_w[half, :, cols]).astype(jnp.bfloat16).astype(jnp.float32)
                for half in range(2)
            ]
            done_buf[pl.ds(first, PLANE), :, cols] = (
                (parts[0] + parts[1]).astype(jnp.bfloat16).reshape(PLANE, CAP, 512)
            )

    def turn(kind, carry):
        for k in range(DEPTH):

            @pl.when(kind == k)
            def _(k=k):
                for i in range(PLANE):
                    if any(ORDER[k][i]):
                        slot = k * PLANE + i
                        pltpu.make_async_copy(
                            recv_buf.at[slot], recv_buf.at[slot], go_got.at[slot]
                        ).wait()

        expert_group(kind, carry)
        for k in range(DEPTH):

            @pl.when(kind == k)
            def _(k=k):
                for i in range(PLANE):
                    if any(ORDER[k][i]):
                        back_copy(k, i).start()

        return carry

    lax.fori_loop(0, DEPTH, turn, 0)
    mine_back = pltpu.make_async_copy(done_buf.at[OWN_SLOT], back_buf.at[sp], own_copy)
    mine_back.start()

    expert_col = lax.broadcasted_iota(jnp.int32, (HALF, EXPERTS), 1)
    routes = [ids_t.astype(jnp.float32), route_ref[...], jnp.zeros((HALF - 4, HALF), jnp.float32)]
    routes = jnp.concatenate(routes, axis=0).T
    ids = routes[:, :2].astype(jnp.int32)
    hot = [(expert_col == ids[:, k : k + 1]).astype(jnp.float32) for k in range(2)]
    earlier = nn(
        (at_col < at_row).astype(jnp.float32).astype(jnp.bfloat16), (hot[0] + hot[1]).astype(jnp.bfloat16)
    )
    slot_col = lax.broadcasted_iota(jnp.int32, (HALF, EXPERTS * CAP), 1)
    takers = []
    for k in range(2):
        rank = jnp.sum(hot[k] * earlier, axis=1, keepdims=True).astype(jnp.int32)
        slot = ids[:, k : k + 1] * CAP + rank
        takers.append((slot_col == slot).astype(jnp.float32).astype(jnp.bfloat16))

    mine_back.wait()

    def await_back(step, carry):
        source = (sp + step) % EXPERTS
        pltpu.make_async_copy(
            back_buf.at[source], back_buf.at[source], back_got.at[source]
        ).wait()
        return carry

    lax.fori_loop(1, EXPERTS, await_back, 0)
    for n in range(4):
        cols = slice(512 * n, 512 * n + 512)
        came = back_buf[:, :, cols].reshape(EXPERTS * CAP, 512)
        both = (
            nn(takers[0], came) * routes[:, 2:3] + nn(takers[1], came) * routes[:, 3:4]
        )
        out_ref[:, cols] = (middle[:, cols].astype(jnp.float32) + both).astype(jnp.bfloat16)

    for copy in next_z:
        copy.wait_send()
    for copy in weight_copies:
        copy.wait_send()
    heads_copy.wait_send()

    for k in (1, 2, 3):
        for kind in range(2):
            first_copy(kind, k).wait_send()
            for j in range(DEPTH):
                second_copy(kind, k, j).wait_send()

        @pl.when(tp == 1)
        def _():
            first_copy(2, k).wait_send()

    def pass_done(source, carry):
        pass_copy(0, source).wait_send()
        pass_copy(1, source).wait_send()
        return carry

    lax.fori_loop(0, PLANE, pass_done, 0)

    for kind, i in away:
        go_copy(kind, i).wait_send()
        back_copy(kind, i).wait_send()


def local(
    residual,
    queries,
    latent,
    rope_key,
    doc_ids,
    latent_to_key,
    latent_to_value,
    out_proj,
    mix_gain,
    moe_gain,
    expert_ids,
    route_weight,
    gate_weight,
    up_weight,
    down_weight,
):
    bf16, f32 = jnp.bfloat16, jnp.float32
    first = lax.axis_index("sp") * ROWS
    positions = (first + jnp.arange(ROWS, dtype=jnp.int32)).astype(f32)
    half_width = ROPE // 2
    frequency = rope_base ** (-jnp.arange(half_width, dtype=f32) / half_width)
    angles = positions[None, :] * frequency[:, None]

    vmem = pl.BlockSpec(memory_space=pltpu.VMEM)
    anywhere = pl.BlockSpec(memory_space=pl.ANY)
    dma = pltpu.SemaphoreType.DMA
    return pl.pallas_call(
        kernel,
        out_shape=jax.ShapeDtypeStruct((HALF, D), bf16),
        in_specs=[vmem] * 13 + [anywhere] * 4,
        out_specs=vmem,
        scratch_shapes=[
            pltpu.VMEM((2, PIECE, LATENT), bf16),
            pltpu.VMEM((HEADS, 128, ROWS), bf16),
            pltpu.VMEM((HEADS * 64, LATENT), bf16),
            pltpu.VMEM((3, PLANE, 2, PIECE, LATENT), bf16),
            pltpu.VMEM((HEADS, 1, ROWS), f32),
            pltpu.VMEM((2, GROUP, STEP, ROWS), f32),
            pltpu.VMEM((2, GROUP, 1, ROWS), f32),
            pltpu.VMEM((HEADS, 1, ROWS), f32),
            pltpu.VMEM((2, GROUP, STEP, ROWS), bf16),
            pltpu.VMEM((HEADS, STEP, 128), bf16),
            pltpu.VMEM((2, HEADS, 80, STEP), bf16),
            pltpu.VMEM((HEADS, 80, ROWS), f32),
            pltpu.VMEM((2, HEADS * 64, HALF), bf16),
            pltpu.VMEM((2, HEADS * 64, HALF), bf16),
            pltpu.VMEM((2 * HEADS * 64, D), bf16),
            pltpu.VMEM((2, D, FF_HALF), bf16),
            pltpu.VMEM((2, D, FF_HALF), bf16),
            pltpu.VMEM((2, FF_HALF, D), bf16),
            pltpu.VMEM((HALF, D), f32),
            pltpu.VMEM((HALF, D), bf16),
            pltpu.VMEM((HALF, D), bf16),
            pltpu.VMEM((EXPERTS, CAP, D), bf16),
            pltpu.VMEM((EXPERTS, CAP, D), bf16),
            pltpu.VMEM((EXPERTS, CAP, D), bf16),
            pltpu.VMEM((EXPERTS, CAP, D), bf16),
            dma((2,)),
            dma((3, DEPTH)),
            dma((2, DEPTH, DEPTH)),
            dma((2, PLANE)),
            dma((3, PLANE)),
            dma((2, PLANE)),
            dma((4,)),
            dma((3,)),
            dma((3,)),
            dma,
            dma,
            dma((EXPERTS,)),
            dma((EXPERTS,)),
            dma,
            dma((EXPERTS,)),
            dma((EXPERTS,)),
        ],
        compiler_params=pltpu.CompilerParams(
            collective_id=0, has_side_effects=True, vmem_limit_bytes=60 * 1024 * 1024
        ),
    )(
        queries.T,
        latent,
        rope_key.T,
        doc_ids.reshape(1, ROWS),
        jnp.cos(angles),
        jnp.sin(angles),
        latent_to_key,
        latent_to_value,
        residual,
        mix_gain.reshape(1, D),
        moe_gain.reshape(1, D),
        expert_ids.T,
        route_weight.T,
        out_proj,
        gate_weight,
        up_weight,
        down_weight,
    )


def solution(mesh):
    in_specs = (
        P(("sp", "tp"), None),
        P("sp", "tp"),
        P("sp", None),
        P("sp", None),
        P("sp"),
        P(None, "tp"),
        P(None, "tp"),
        P(),
        P(),
        P(),
        P(("sp", "tp"), None),
        P(("sp", "tp"), None),
        P("sp", None, "tp"),
        P("sp", None, "tp"),
        P("sp", "tp", None),
    )
    out_specs = P(("sp", "tp"), None)
    return jax.shard_map(local, mesh=mesh, in_specs=in_specs, out_specs=out_specs, check_vma=False)
```

```python
import functools

import jax
import jax.numpy as jnp
from jax import lax
from jax.experimental import pallas as pl
from jax.experimental.pallas import tpu as pltpu
from jax.sharding import PartitionSpec as P

D = 2048
UNROTATED_DIM = 64
ROPE = 32
HEADS = 6
LATENT = 256
ROWS = 256
HALF = 128
PIECE = 160
EXPERTS = 64
CAP = 8
FF_HALF = 512
PLANE = 16
DEPTH = 4
GROUP = 2
GROUPS = HEADS // GROUP
CHUNK = 64
STEP = 4 * ROWS
DEAD = 40
rope_base = 10000.0
epsilon = 1e-06
MASKED = 1e30
SCORE_BASE2 = float((UNROTATED_DIM + ROPE) ** (-0.5) * 1.4426950408889634)
MESH = pl.DeviceIdType.MESH


def hops(offset):
    return [min(v, DEPTH - v) for v in offset]


def exchange_order():
    cube = [(a, b, c) for a in range(DEPTH) for b in range(DEPTH) for c in range(DEPTH)]
    classes = []
    for kind in range(DEPTH):
        left = [o for o in cube if sum(o) % DEPTH == kind and any(o)]
        order, load = [], [0, 0, 0]
        while left:
            best = min(
                left,
                key=lambda o: (
                    max(a + b for a, b in zip(load, hops(o))) - min(a + b for a, b in zip(load, hops(o))),
                    -sum(hops(o)),
                    o,
                ),
            )
            left.remove(best)
            order.append(best)
            load = [a + b for a, b in zip(load, hops(best))]
        classes.append(order if kind else order + [(0, 0, 0)])
    return classes


ORDER = exchange_order()
OWN_SLOT = PLANE - 1
SEQUENCE = [(0, 0), (0, 1), (1, 0), (0, 3), (3, 0), (0, 2), (2, 0), (1, 1)]
SEQUENCE += [(1, 3), (3, 1), (3, 3), (1, 2), (2, 1), (3, 2), (2, 3), (2, 2)]


def turned(upper, lower, cosine, sine_part):
    return [upper * cosine - lower * sine_part, lower * cosine + upper * sine_part]


def nn(a, b):
    return lax.dot_general(a, b, (((1,), (0,)), ((), ())), preferred_element_type=jnp.float32)


def nt(a, b):
    return lax.dot_general(a, b, (((1,), (1,)), ((), ())), preferred_element_type=jnp.float32)


def kernel(
    raw_query_ref,
    latent_ref,
    rope_ref,
    doc_ref,
    cosine_ref,
    sine_ref,
    key_w_ref,
    raw_value_w_ref,
    residual_ref,
    mix_gain_ref,
    moe_gain_ref,
    ids_ref,
    route_ref,
    proj_hbm,
    gate_hbm,
    up_hbm,
    down_hbm,
    out_ref,
    own_ref,
    query_ref,
    value_w_ref,
    kv,
    run_max,
    held,
    tops,
    factors,
    probs,
    full_keys,
    values,
    run_out,
    turned_out,
    heads_buf,
    proj,
    gate_w,
    up_w,
    down_w,
    mix,
    middle,
    normed,
    send_buf,
    recv_buf,
    done_buf,
    back_buf,
    z_send,
    first_send,
    second_send,
    pass_send,
    got,
    passed,
    weight_local,
    weight_send,
    weight_got,
    heads_send,
    heads_got,
    go_send,
    go_got,
    own_copy,
    back_send,
    back_got,
):
    sp = lax.axis_index("sp")
    tp = lax.axis_index("tp")
    other = 1 - tp
    z = sp // PLANE
    me = sp % PLANE
    y, x = me // DEPTH, me % DEPTH

    def remote(src, dst, send_sem, recv_sem, device):
        return pltpu.make_async_remote_copy(
            src_ref=src,
            dst_ref=dst,
            send_sem=send_sem,
            recv_sem=recv_sem,
            device_id=device,
            device_id_type=MESH,
        )

    barrier = pltpu.get_barrier_semaphore()
    pl.semaphore_signal(barrier, inc=1, device_id=(sp, other), device_id_type=MESH)

    def greet(step, carry):
        pl.semaphore_signal(
            barrier, inc=1, device_id=((sp + step) % EXPERTS, tp), device_id_type=MESH
        )
        return carry

    lax.fori_loop(1, EXPERTS, greet, 0)

    local_copies = [
        pltpu.make_async_copy(proj_hbm, proj, weight_local.at[0]),
        pltpu.make_async_copy(gate_hbm.at[0], gate_w.at[tp], weight_local.at[1]),
        pltpu.make_async_copy(up_hbm.at[0], up_w.at[tp], weight_local.at[2]),
        pltpu.make_async_copy(down_hbm.at[0], down_w.at[tp], weight_local.at[3]),
    ]
    for copy in local_copies:
        copy.start()

    cosine, sine_part = cosine_ref[...], sine_ref[...]
    rope = rope_ref[...].astype(jnp.float32)
    hot = (lax.broadcasted_iota(jnp.int32, (8, ROWS), 0) == doc_ref[...]).astype(jnp.float32)
    extra = turned(rope[:16, :], rope[16:, :], cosine, sine_part) + [hot, jnp.zeros((24, ROWS), jnp.float32)]
    extra = jnp.concatenate(extra + extra, axis=0).T.astype(jnp.bfloat16)
    low_quarter = lax.broadcasted_iota(jnp.int32, (PIECE - HALF, 128), 1) < 64
    for half in range(2):
        own_ref[half, :HALF, :] = latent_ref[HALF * half : HALF * half + HALF, :]
        for tile in range(2):
            at = HALF * half + 64 * tile
            own_ref[half, HALF:PIECE, 128 * tile : 128 * tile + 128] = jnp.where(
                low_quarter, extra[at : at + 32, :], extra[at + 32 : at + 64, :]
            )
    keep = pltpu.make_async_copy(own_ref.at[tp], kv.at[2, me, tp], own_copy)
    keep.start()
    keep.wait()
    pl.semaphore_wait(barrier, EXPERTS)

    next_z = []
    for hop in (1, 2):
        target = ((z + hop) % DEPTH) * PLANE + me
        copy = remote(
            own_ref.at[tp],
            kv.at[hop - 1, me, tp],
            z_send.at[hop - 1],
            got.at[hop - 1, me],
            (target, tp),
        )
        copy.start()
        next_z.append(copy)

    def place(dy, dx):
        return ((y + dy + DEPTH) % DEPTH) * DEPTH + (x + dx + DEPTH) % DEPTH

    def first_peer(k):
        return jnp.where(tp == 0, place(k, 0), place(0, k))

    def second_peer(k):
        return jnp.where(tp == 0, place(0, k), place(k, 0))

    def first_copy(kind, k):
        peer = first_peer(k)
        later = peer > me
        source = (0, jnp.where(later, 2, 1), jnp.where(later, 1, 2))[kind]
        return remote(
            kv.at[source, me, tp],
            kv.at[kind, me, tp],
            first_send.at[kind, k],
            got.at[kind, me],
            (z * PLANE + peer, tp),
        )

    def second_copy(kind, k, j):
        peer = second_peer(k)
        later = peer > me
        origin = first_peer(-j)
        if kind == 0:
            source = 0
        elif j == 0:
            source = jnp.where(later, 2, 1)
        else:
            source = jnp.where((tp == 1) & ((origin < me) != later), 2, 1)
        return remote(
            kv.at[source, origin, tp],
            kv.at[kind, origin, tp],
            second_send.at[kind, k, j],
            got.at[kind, origin],
            (z * PLANE + peer, tp),
        )

    weight_copies = [
        remote(src.at[0], dst.at[tp], weight_send.at[i], weight_got.at[i], (sp, other))
        for i, (src, dst) in enumerate(((gate_hbm, gate_w), (up_hbm, up_w), (down_hbm, down_w)))
    ]
    for copy in weight_copies:
        copy.start()

    mask = (hot - 1.0) * MASKED
    dead_row = jnp.where(lax.broadcasted_iota(jnp.int32, (24, ROWS), 0) == 0, -MASKED, 0.0)
    flat = raw_query_ref[...].astype(jnp.float32)
    for head in range(HEADS):
        at = (UNROTATED_DIM + ROPE) * head
        plain = [flat[at : at + 64, :]]
        rest = turned(flat[at + 64 : at + 80, :], flat[at + 80 : at + 96, :], cosine, sine_part)
        rest = rest + [mask, dead_row]
        query_ref[head] = jnp.concatenate(
            plain + rest if head % 2 == 0 else rest + plain, axis=0
        ).astype(jnp.bfloat16)
    value_w_ref[...] = raw_value_w_ref[...].astype(jnp.float32).T.astype(jnp.bfloat16)
    values[...] = jnp.ones_like(values)
    low_lanes = lax.broadcasted_iota(jnp.int32, (HALF, 128), 1) < 64
    dead_lane = (lax.broadcasted_iota(jnp.int32, (PIECE - HALF, 128), 1) % 64 == DEAD).astype(
        jnp.float32
    )

    def project(blocks, dead, bank):
        for number, (block, flag) in enumerate(zip(blocks, dead)):
            at = ROWS * number
            for half in range(2):
                low, high = [], []
                for tile in range(2):
                    extra = block[half, HALF:PIECE, 128 * tile : 128 * tile + 128].astype(jnp.float32)
                    if flag is not None:
                        extra = extra + dead_lane * flag
                    swapped = pltpu.roll(extra, 64, 1)
                    low += [extra, swapped]
                    high += [swapped, extra]
                low = jnp.concatenate(low, axis=0).astype(jnp.bfloat16)
                high = jnp.concatenate(high, axis=0).astype(jnp.bfloat16)
                keys = nn(block[half, :HALF, :], key_w_ref[...]).astype(jnp.bfloat16)
                for head in range(HEADS):
                    column = keys[:, 128 * (head // 2) : 128 * (head // 2) + 128]
                    if head % 2 == 0:
                        full_key = jnp.where(low_lanes, column, high)
                    else:
                        full_key = jnp.where(low_lanes, low, column)
                    full_keys[head, at + HALF * half : at + HALF * half + HALF, :] = full_key
            rows = jnp.concatenate([block[0, :HALF, :], block[1, :HALF, :]], axis=0)
            every = nt(value_w_ref[...], rows).astype(jnp.bfloat16)
            for head in range(HEADS):
                values[bank, head, :64, at : at + ROWS] = every[64 * head : 64 * head + 64, :]

    def score(first, slot, keys_at, causal):
        for i in range(GROUP):
            head = first + i
            top = None
            for number in range(keys_at // HALF):
                at = HALF * number
                scores = nn(full_keys[head, at : at + HALF, :], query_ref[head])
                if causal:
                    key_at = lax.broadcasted_iota(jnp.int32, (HALF, ROWS), 0) + at
                    query_at = lax.broadcasted_iota(jnp.int32, (HALF, ROWS), 1)
                    scores = jnp.where(key_at <= query_at, scores, -MASKED)
                held[slot, i, at : at + HALF, :] = scores
                here = jnp.max(scores.reshape(HALF // 8, 8, ROWS), axis=0)
                top = here if top is None else jnp.maximum(top, here)
            tops[slot, i] = jnp.max(top, axis=0, keepdims=True)

    def weigh(first, slot, keys_at, causal):
        for i in range(GROUP):
            head = first + i
            if causal:
                new_max = tops[slot, i]
            else:
                old_max = run_max[head]
                new_max = jnp.maximum(old_max, tops[slot, i])
                factors[head] = jnp.exp2((old_max - new_max) * SCORE_BASE2)
            run_max[head] = new_max
            for number in range(keys_at // CHUNK):
                at = CHUNK * number
                probs[slot, i, at : at + CHUNK, :] = jnp.exp2(
                    (held[slot, i, at : at + CHUNK, :] - new_max) * SCORE_BASE2
                ).astype(jnp.bfloat16)

    def gather_values(first, slot, keys_at, bank, causal):
        for i in range(GROUP):
            head = first + i
            part = nn(values[bank, head, :, :keys_at], probs[slot, i, :keys_at, :])
            if causal:
                run_out[head] = part
            else:
                run_out[head] = run_out[head] * factors[head] + part

    project([own_ref], [None], 1)
    for j in range(GROUPS):
        score(j * GROUP, j % 2, ROWS, True)
        weigh(j * GROUP, j % 2, ROWS, True)
        gather_values(j * GROUP, j % 2, ROWS, 1, True)

    def pass_copy(kind, source):
        return remote(
            kv.at[kind, source, tp],
            kv.at[kind, source, tp],
            pass_send.at[kind, source],
            passed.at[kind, source],
            (sp, other),
        )

    def arrival(kind, source):
        return pltpu.make_async_copy(
            kv.at[kind, source, tp], kv.at[kind, source, tp], got.at[kind, source]
        )

    def take(origin):
        for kind in range(2):
            arrival(kind, origin).wait()
            pass_copy(kind, origin).start()

    def relay(j):
        origin = first_peer(-j)
        take(origin)

        @pl.when(tp == 1)
        def _():
            arrival(2, origin).wait()

        for k in (1, 3, 2):
            for kind in range(2):
                second_copy(kind, k, j).start()

    take(me)
    for k in (1, 3):
        for kind in range(2):
            first_copy(kind, k).start()
            second_copy(kind, k, 0).start()

    @pl.when(tp == 1)
    def _():
        for k in (1, 3):
            first_copy(2, k).start()

    for kind in range(2):
        first_copy(kind, 2).start()
        second_copy(kind, 2, 0).start()

    @pl.when(tp == 1)
    def _():
        first_copy(2, 2).start()

    for j in (1, 3):
        relay(j)
        take(second_peer(-j))

    last_slot = (GROUPS - 1) % 2
    last_head = (GROUPS - 1) * GROUP

    def errands(step):
        @pl.when(step == 0)
        def _():
            relay(2)
            take(second_peer(-2))

        for n in range(1, len(SEQUENCE) // 2 - 1):
            ahead = [o for o in SEQUENCE[2 * n + 2 : 2 * n + 4] if o[0] and o[1]]
            if ahead:

                @pl.when(step == n)
                def _(ahead=ahead):
                    for dy, dx in ahead:
                        take(place(-dy, -dx))

    def visit(step, carry):
        sources = []
        for i in range(2):
            dy, dx = 0, 0
            for n in range(len(SEQUENCE) // 2):
                dy = jnp.where(step == n, SEQUENCE[2 * n + i][0], dy)
                dx = jnp.where(step == n, SEQUENCE[2 * n + i][1], dx)
            sources.append(place(-dy, -dx))

        for source in sources:
            for kind in range(2):
                pltpu.make_async_copy(
                    kv.at[kind, source, other], kv.at[kind, source, other], passed.at[kind, source]
                ).wait()

        @pl.when(step >= 0)
        def _():
            bank = step % 2
            blocks, dead = [], []
            for source in sources:
                blocks += [kv.at[0, source], kv.at[1, source]]
                dead += [
                    (z < 1).astype(jnp.float32),
                    ((source >= me) & (z < 2)).astype(jnp.float32),
                ]

            project(blocks, dead, bank)
            score(0, 0, STEP, False)

            for j in range(GROUPS - 1):
                if j == 1:
                    errands(step)

                @pl.when(step >= -1 - j)
                def _(j=j):
                    if j > 0:
                        gather_values((j - 1) * GROUP, (j - 1) % 2, STEP, bank, False)
                    weigh(j * GROUP, j % 2, STEP, False)
                    score((j + 1) * GROUP, (j + 1) % 2, STEP, False)

            gather_values(last_head - GROUP, (last_slot + 1) % 2, STEP, bank, False)
            weigh(last_head, last_slot, STEP, False)
            gather_values(last_head, last_slot, STEP, bank, False)

        return carry

    lax.fori_loop(0, PLANE // 2, visit, 0)

    for head in range(HEADS):
        done = (run_out[head, :64, :] / run_out[head, 64:65, :]).astype(jnp.bfloat16)
        for part in range(2):
            turned_out[part, 64 * head : 64 * head + 64, :] = done[:, HALF * part : HALF * part + HALF]
    heads_copy = remote(
        turned_out.at[other], heads_buf.at[tp], heads_send, heads_got, (sp, other)
    )
    heads_copy.start()
    heads_buf[tp] = turned_out[tp]
    local_copies[0].wait()
    heads_copy.wait_recv()

    attended = jnp.concatenate(
        [heads_buf[g].astype(jnp.float32).T.astype(jnp.bfloat16) for g in range(2)], axis=1
    )
    squares = jnp.zeros((HALF, 1), jnp.float32)
    for n in range(4):
        cols = slice(512 * n, 512 * n + 512)
        part = nn(attended, proj[:, cols])
        mix[:, cols] = part
        squares = squares + jnp.sum(part * part, axis=1, keepdims=True)
    scale = lax.rsqrt(squares * (1.0 / D) + epsilon)
    squares = jnp.zeros((HALF, 1), jnp.float32)
    for n in range(4):
        cols = slice(512 * n, 512 * n + 512)
        branch = mix[:, cols] * scale * mix_gain_ref[:, cols]
        mid = (residual_ref[:, cols].astype(jnp.float32) + branch).astype(jnp.bfloat16)
        middle[:, cols] = mid
        wide = mid.astype(jnp.float32)
        squares = squares + jnp.sum(wide * wide, axis=1, keepdims=True)
    scale = lax.rsqrt(squares * (1.0 / D) + epsilon)
    for n in range(4):
        cols = slice(512 * n, 512 * n + 512)
        normed[:, cols] = (
            middle[:, cols].astype(jnp.float32) * scale * moe_gain_ref[:, cols]
        ).astype(jnp.bfloat16)

    at_row = lax.broadcasted_iota(jnp.int32, (HALF, HALF), 0)
    at_col = lax.broadcasted_iota(jnp.int32, (HALF, HALF), 1)
    expert_row = lax.broadcasted_iota(jnp.int32, (EXPERTS, HALF), 0)
    ids_t = ids_ref[...]
    hot = [(expert_row == ids_t[k : k + 1, :]).astype(jnp.float32) for k in range(2)]
    earlier = nn(
        (hot[0] + hot[1]).astype(jnp.bfloat16), (at_row < at_col).astype(jnp.float32).astype(jnp.bfloat16)
    )
    slot_row = lax.broadcasted_iota(jnp.int32, (EXPERTS * CAP, HALF), 0)
    chooser = jnp.zeros((EXPERTS * CAP, HALF), jnp.float32)
    for k in range(2):
        rank = jnp.sum(hot[k] * earlier, axis=0, keepdims=True).astype(jnp.int32)
        slot = ids_t[k : k + 1, :] * CAP + rank
        chooser = chooser + (slot_row == slot).astype(jnp.float32)
    chooser = chooser.astype(jnp.bfloat16)
    for n in range(8):
        cols = slice(256 * n, 256 * n + 256)
        picked = nn(chooser, normed[:, cols]).astype(jnp.bfloat16)
        send_buf[:, :, cols] = picked.reshape(EXPERTS, CAP, 256)

    def toward(offset, sign):
        dz, dy, dx = offset
        return (
            ((z + sign * dz + DEPTH) % DEPTH) * PLANE
            + ((y + sign * dy + DEPTH) % DEPTH) * DEPTH
            + (x + sign * dx + DEPTH) % DEPTH
        )

    def go_copy(kind, i):
        target = toward(ORDER[kind][i], 1)
        slot = kind * PLANE + i
        return remote(
            send_buf.at[target], recv_buf.at[slot], go_send.at[slot], go_got.at[slot], (target, tp)
        )

    def back_copy(kind, i):
        source = toward(ORDER[kind][i], -1)
        slot = kind * PLANE + i
        return remote(
            done_buf.at[slot], back_buf.at[sp], back_send.at[slot], back_got.at[sp], (source, tp)
        )

    away = [(kind, i) for kind in range(DEPTH) for i in range(PLANE) if any(ORDER[kind][i])]
    for kind, i in away:
        go_copy(kind, i).start()
    mine = pltpu.make_async_copy(send_buf.at[sp], recv_buf.at[OWN_SLOT], own_copy)
    mine.start()
    for copy in local_copies[1:]:
        copy.wait()
    for copy in weight_copies:
        copy.wait_recv()
    mine.wait()

    def expert_group(kind, carry):
        first = kind * PLANE
        rows = recv_buf[pl.ds(first, PLANE)].reshape(PLANE * CAP, D)
        hidden = []
        for half in range(2):
            gate_out = nn(rows, gate_w[half])
            up_out = nn(rows, up_w[half])
            hidden.append((gate_out / (1.0 + jnp.exp(-gate_out)) * up_out).astype(jnp.bfloat16))
        for n in range(4):
            cols = slice(512 * n, 512 * n + 512)
            parts = [
                nn(hidden[half], down_w[half, :, cols]).astype(jnp.bfloat16).astype(jnp.float32)
                for half in range(2)
            ]
            done_buf[pl.ds(first, PLANE), :, cols] = (
                (parts[0] + parts[1]).astype(jnp.bfloat16).reshape(PLANE, CAP, 512)
            )

    def turn(kind, carry):
        for k in range(DEPTH):

            @pl.when(kind == k)
            def _(k=k):
                for i in range(PLANE):
                    if any(ORDER[k][i]):
                        slot = k * PLANE + i
                        pltpu.make_async_copy(
                            recv_buf.at[slot], recv_buf.at[slot], go_got.at[slot]
                        ).wait()

        expert_group(kind, carry)
        for k in range(DEPTH):

            @pl.when(kind == k)
            def _(k=k):
                for i in range(PLANE):
                    if any(ORDER[k][i]):
                        back_copy(k, i).start()

        return carry

    lax.fori_loop(0, DEPTH, turn, 0)
    mine_back = pltpu.make_async_copy(done_buf.at[OWN_SLOT], back_buf.at[sp], own_copy)
    mine_back.start()

    expert_col = lax.broadcasted_iota(jnp.int32, (HALF, EXPERTS), 1)
    routes = [ids_t.astype(jnp.float32), route_ref[...], jnp.zeros((HALF - 4, HALF), jnp.float32)]
    routes = jnp.concatenate(routes, axis=0).T
    ids = routes[:, :2].astype(jnp.int32)
    hot = [(expert_col == ids[:, k : k + 1]).astype(jnp.float32) for k in range(2)]
    earlier = nn(
        (at_col < at_row).astype(jnp.float32).astype(jnp.bfloat16), (hot[0] + hot[1]).astype(jnp.bfloat16)
    )
    slot_col = lax.broadcasted_iota(jnp.int32, (HALF, EXPERTS * CAP), 1)
    takers = []
    for k in range(2):
        rank = jnp.sum(hot[k] * earlier, axis=1, keepdims=True).astype(jnp.int32)
        slot = ids[:, k : k + 1] * CAP + rank
        takers.append((slot_col == slot).astype(jnp.float32).astype(jnp.bfloat16))

    mine_back.wait()

    def await_back(step, carry):
        source = (sp + step) % EXPERTS
        pltpu.make_async_copy(
            back_buf.at[source], back_buf.at[source], back_got.at[source]
        ).wait()
        return carry

    lax.fori_loop(1, EXPERTS, await_back, 0)
    for n in range(4):
        cols = slice(512 * n, 512 * n + 512)
        came = back_buf[:, :, cols].reshape(EXPERTS * CAP, 512)
        both = (
            nn(takers[0], came) * routes[:, 2:3] + nn(takers[1], came) * routes[:, 3:4]
        )
        out_ref[:, cols] = (middle[:, cols].astype(jnp.float32) + both).astype(jnp.bfloat16)

    for copy in next_z:
        copy.wait_send()
    for copy in weight_copies:
        copy.wait_send()
    heads_copy.wait_send()

    for k in (1, 2, 3):
        for kind in range(2):
            first_copy(kind, k).wait_send()
            for j in range(DEPTH):
                second_copy(kind, k, j).wait_send()

        @pl.when(tp == 1)
        def _():
            first_copy(2, k).wait_send()

    def pass_done(source, carry):
        pass_copy(0, source).wait_send()
        pass_copy(1, source).wait_send()
        return carry

    lax.fori_loop(0, PLANE, pass_done, 0)

    for kind, i in away:
        go_copy(kind, i).wait_send()
        back_copy(kind, i).wait_send()


def local(
    residual,
    queries,
    latent,
    rope_key,
    doc_ids,
    latent_to_key,
    latent_to_value,
    out_proj,
    mix_gain,
    moe_gain,
    expert_ids,
    route_weight,
    gate_weight,
    up_weight,
    down_weight,
):
    bf16, f32 = jnp.bfloat16, jnp.float32
    first = lax.axis_index("sp") * ROWS
    positions = (first + jnp.arange(ROWS, dtype=jnp.int32)).astype(f32)
    half_width = ROPE // 2
    frequency = rope_base ** (-jnp.arange(half_width, dtype=f32) / half_width)
    angles = positions[None, :] * frequency[:, None]

    vmem = pl.BlockSpec(memory_space=pltpu.VMEM)
    anywhere = pl.BlockSpec(memory_space=pl.ANY)
    dma = pltpu.SemaphoreType.DMA
    return pl.pallas_call(
        kernel,
        out_shape=pltpu.VMEM((HALF, D), bf16),
        in_specs=[vmem] * 13 + [anywhere] * 4,
        out_specs=vmem,
        scratch_shapes=[
            pltpu.VMEM((2, PIECE, LATENT), bf16),
            pltpu.VMEM((HEADS, 128, ROWS), bf16),
            pltpu.VMEM((HEADS * 64, LATENT), bf16),
            pltpu.VMEM((3, PLANE, 2, PIECE, LATENT), bf16),
            pltpu.VMEM((HEADS, 1, ROWS), f32),
            pltpu.VMEM((2, GROUP, STEP, ROWS), f32),
            pltpu.VMEM((2, GROUP, 1, ROWS), f32),
            pltpu.VMEM((HEADS, 1, ROWS), f32),
            pltpu.VMEM((2, GROUP, STEP, ROWS), bf16),
            pltpu.VMEM((HEADS, STEP, 128), bf16),
            pltpu.VMEM((2, HEADS, 80, STEP), bf16),
            pltpu.VMEM((HEADS, 80, ROWS), f32),
            pltpu.VMEM((2, HEADS * 64, HALF), bf16),
            pltpu.VMEM((2, HEADS * 64, HALF), bf16),
            pltpu.VMEM((2 * HEADS * 64, D), bf16),
            pltpu.VMEM((2, D, FF_HALF), bf16),
            pltpu.VMEM((2, D, FF_HALF), bf16),
            pltpu.VMEM((2, FF_HALF, D), bf16),
            pltpu.VMEM((HALF, D), f32),
            pltpu.VMEM((HALF, D), bf16),
            pltpu.VMEM((HALF, D), bf16),
            pltpu.VMEM((EXPERTS, CAP, D), bf16),
            pltpu.VMEM((EXPERTS, CAP, D), bf16),
            pltpu.VMEM((EXPERTS, CAP, D), bf16),
            pltpu.VMEM((EXPERTS, CAP, D), bf16),
            dma((2,)),
            dma((3, DEPTH)),
            dma((2, DEPTH, DEPTH)),
            dma((2, PLANE)),
            dma((3, PLANE)),
            dma((2, PLANE)),
            dma((4,)),
            dma((3,)),
            dma((3,)),
            dma,
            dma,
            dma((EXPERTS,)),
            dma((EXPERTS,)),
            dma,
            dma((EXPERTS,)),
            dma((EXPERTS,)),
        ],
        compiler_params=pltpu.CompilerParams(
            collective_id=0, has_side_effects=True, vmem_limit_bytes=60 * 1024 * 1024
        ),
    )(
        queries.T,
        latent,
        rope_key.T,
        doc_ids.reshape(1, ROWS),
        jnp.cos(angles),
        jnp.sin(angles),
        latent_to_key,
        latent_to_value,
        residual,
        mix_gain.reshape(1, D),
        moe_gain.reshape(1, D),
        expert_ids.T,
        route_weight.T,
        out_proj,
        gate_weight,
        up_weight,
        down_weight,
    )


def solution(mesh):
    in_specs = (
        P(("sp", "tp"), None),
        P("sp", "tp"),
        P("sp", None),
        P("sp", None),
        P("sp"),
        P(None, "tp"),
        P(None, "tp"),
        P(),
        P(),
        P(),
        P(("sp", "tp"), None),
        P(("sp", "tp"), None),
        P("sp", None, "tp"),
        P("sp", None, "tp"),
        P("sp", "tp", None),
    )
    out_specs = P(("sp", "tp"), None)
    return jax.shard_map(local, mesh=mesh, in_specs=in_specs, out_specs=out_specs, check_vma=False)
```

```python
import functools

import jax
import jax.numpy as jnp
from jax import lax
from jax.experimental import pallas as pl
from jax.experimental.pallas import tpu as pltpu
from jax.sharding import PartitionSpec as P

D = 2048
UNROTATED_DIM = 64
ROPE = 32
HEADS = 6
LATENT = 256
ROWS = 256
HALF = 128
PIECE = 160
EXPERTS = 64
CAP = 8
FF_HALF = 512
PLANE = 16
DEPTH = 4
GROUP = 2
GROUPS = HEADS // GROUP
CHUNK = 128
STEP = 4 * ROWS
DEAD = 40
rope_base = 10000.0
epsilon = 1e-06
MASKED = 1e30
SCORE_BASE2 = float((UNROTATED_DIM + ROPE) ** (-0.5) * 1.4426950408889634)
MESH = pl.DeviceIdType.MESH


def hops(offset):
    return [min(v, DEPTH - v) for v in offset]


def exchange_order():
    cube = [(a, b, c) for a in range(DEPTH) for b in range(DEPTH) for c in range(DEPTH)]
    classes = []
    for kind in range(DEPTH):
        left = [o for o in cube if sum(o) % DEPTH == kind and any(o)]
        order, load = [], [0, 0, 0]
        while left:
            best = min(
                left,
                key=lambda o: (
                    max(a + b for a, b in zip(load, hops(o))) - min(a + b for a, b in zip(load, hops(o))),
                    -sum(hops(o)),
                    o,
                ),
            )
            left.remove(best)
            order.append(best)
            load = [a + b for a, b in zip(load, hops(best))]
        classes.append(order if kind else order + [(0, 0, 0)])
    return classes


ORDER = exchange_order()
OWN_SLOT = PLANE - 1
SEQUENCE = [(0, 0), (0, 1), (1, 0), (0, 3), (3, 0), (0, 2), (2, 0), (1, 1)]
SEQUENCE += [(1, 3), (3, 1), (3, 3), (1, 2), (2, 1), (3, 2), (2, 3), (2, 2)]


def turned(upper, lower, cosine, sine_part):
    return [upper * cosine - lower * sine_part, lower * cosine + upper * sine_part]


def nn(a, b):
    return lax.dot_general(a, b, (((1,), (0,)), ((), ())), preferred_element_type=jnp.float32)


def nt(a, b):
    return lax.dot_general(a, b, (((1,), (1,)), ((), ())), preferred_element_type=jnp.float32)


def kernel(
    raw_query_ref,
    latent_ref,
    rope_ref,
    doc_ref,
    cosine_ref,
    sine_ref,
    key_w_ref,
    raw_value_w_ref,
    residual_ref,
    mix_gain_ref,
    moe_gain_ref,
    ids_ref,
    route_ref,
    proj_hbm,
    gate_hbm,
    up_hbm,
    down_hbm,
    out_ref,
    own_ref,
    query_ref,
    value_w_ref,
    kv,
    run_max,
    held,
    tops,
    factors,
    probs,
    full_keys,
    values,
    run_out,
    turned_out,
    heads_buf,
    proj,
    gate_w,
    up_w,
    down_w,
    mix,
    middle,
    normed,
    send_buf,
    recv_buf,
    done_buf,
    back_buf,
    z_send,
    first_send,
    second_send,
    pass_send,
    got,
    passed,
    weight_local,
    weight_send,
    weight_got,
    heads_send,
    heads_got,
    go_send,
    go_got,
    own_copy,
    back_send,
    back_got,
    plane_in,
    all_in,
):
    sp = lax.axis_index("sp")
    tp = lax.axis_index("tp")
    other = 1 - tp
    z = sp // PLANE
    me = sp % PLANE
    y, x = me // DEPTH, me % DEPTH

    def remote(src, dst, send_sem, recv_sem, device):
        return pltpu.make_async_remote_copy(
            src_ref=src,
            dst_ref=dst,
            send_sem=send_sem,
            recv_sem=recv_sem,
            device_id=device,
            device_id_type=MESH,
        )

    def in_line(axis, k):
        at = [z, y, x]
        at[axis] = (at[axis] + k) % DEPTH
        return (at[0] * PLANE + at[1] * DEPTH + at[2], tp)

    barrier = pltpu.get_barrier_semaphore()
    pl.semaphore_signal(barrier, inc=1, device_id=(sp, other), device_id_type=MESH)
    for axis in range(3):
        for k in range(1, DEPTH):
            pl.semaphore_signal(barrier, inc=1, device_id=in_line(axis, k), device_id_type=MESH)

    local_copies = [
        pltpu.make_async_copy(proj_hbm, proj, weight_local.at[0]),
        pltpu.make_async_copy(gate_hbm.at[0], gate_w.at[tp], weight_local.at[1]),
        pltpu.make_async_copy(up_hbm.at[0], up_w.at[tp], weight_local.at[2]),
        pltpu.make_async_copy(down_hbm.at[0], down_w.at[tp], weight_local.at[3]),
    ]
    for copy in local_copies:
        copy.start()

    cosine, sine_part = cosine_ref[...], sine_ref[...]
    rope = rope_ref[...].astype(jnp.float32)
    hot = (lax.broadcasted_iota(jnp.int32, (8, ROWS), 0) == doc_ref[...]).astype(jnp.float32)
    extra = turned(rope[:16, :], rope[16:, :], cosine, sine_part) + [hot, jnp.zeros((24, ROWS), jnp.float32)]
    extra = jnp.concatenate(extra + extra, axis=0).T.astype(jnp.bfloat16)
    low_quarter = lax.broadcasted_iota(jnp.int32, (PIECE - HALF, 128), 1) < 64
    for half in range(2):
        own_ref[half, :HALF, :] = latent_ref[HALF * half : HALF * half + HALF, :]
        for tile in range(2):
            at = HALF * half + 64 * tile
            own_ref[half, HALF:PIECE, 128 * tile : 128 * tile + 128] = jnp.where(
                low_quarter, extra[at : at + 32, :], extra[at + 32 : at + 64, :]
            )
    keep = pltpu.make_async_copy(own_ref.at[tp], kv.at[2, me, tp], own_copy)
    keep.start()
    keep.wait()
    pl.semaphore_wait(barrier, 3 * (DEPTH - 1) + 1)
    for k in range(1, DEPTH):
        pl.semaphore_signal(plane_in, inc=1, device_id=in_line(2, k), device_id_type=MESH)

    next_z = []
    for hop in (1, 2):
        target = ((z + hop) % DEPTH) * PLANE + me
        copy = remote(
            own_ref.at[tp],
            kv.at[hop - 1, me, tp],
            z_send.at[hop - 1],
            got.at[hop - 1, me],
            (target, tp),
        )
        copy.start()
        next_z.append(copy)

    def place(dy, dx):
        return ((y + dy + DEPTH) % DEPTH) * DEPTH + (x + dx + DEPTH) % DEPTH

    def first_peer(k):
        return jnp.where(tp == 0, place(k, 0), place(0, k))

    def second_peer(k):
        return jnp.where(tp == 0, place(0, k), place(k, 0))

    def first_copy(kind, k):
        peer = first_peer(k)
        later = peer > me
        source = (0, jnp.where(later, 2, 1), jnp.where(later, 1, 2))[kind]
        return remote(
            kv.at[source, me, tp],
            kv.at[kind, me, tp],
            first_send.at[kind, k],
            got.at[kind, me],
            (z * PLANE + peer, tp),
        )

    def second_copy(kind, k, j):
        peer = second_peer(k)
        later = peer > me
        origin = first_peer(-j)
        if kind == 0:
            source = 0
        elif j == 0:
            source = jnp.where(later, 2, 1)
        else:
            source = jnp.where((tp == 1) & ((origin < me) != later), 2, 1)
        return remote(
            kv.at[source, origin, tp],
            kv.at[kind, origin, tp],
            second_send.at[kind, k, j],
            got.at[kind, origin],
            (z * PLANE + peer, tp),
        )

    weight_copies = [
        remote(src.at[0], dst.at[tp], weight_send.at[i], weight_got.at[i], (sp, other))
        for i, (src, dst) in enumerate(((gate_hbm, gate_w), (up_hbm, up_w), (down_hbm, down_w)))
    ]
    for copy in weight_copies:
        copy.start()

    mask = (hot - 1.0) * MASKED
    dead_row = jnp.where(lax.broadcasted_iota(jnp.int32, (24, ROWS), 0) == 0, -MASKED, 0.0)
    flat = raw_query_ref[...].astype(jnp.float32)
    for head in range(HEADS):
        at = (UNROTATED_DIM + ROPE) * head
        plain = [flat[at : at + 64, :]]
        rest = turned(flat[at + 64 : at + 80, :], flat[at + 80 : at + 96, :], cosine, sine_part)
        rest = rest + [mask, dead_row]
        query_ref[head] = jnp.concatenate(
            plain + rest if head % 2 == 0 else rest + plain, axis=0
        ).astype(jnp.bfloat16)
    value_w_ref[...] = raw_value_w_ref[...].astype(jnp.float32).T.astype(jnp.bfloat16)
    values[...] = jnp.ones_like(values)
    low_lanes = lax.broadcasted_iota(jnp.int32, (HALF, 128), 1) < 64
    dead_lane = (lax.broadcasted_iota(jnp.int32, (PIECE - HALF, 128), 1) % 64 == DEAD).astype(
        jnp.float32
    )

    def project(blocks, dead, bank):
        for number, (block, flag) in enumerate(zip(blocks, dead)):
            at = ROWS * number
            for half in range(2):
                low, high = [], []
                for tile in range(2):
                    extra = block[half, HALF:PIECE, 128 * tile : 128 * tile + 128].astype(jnp.float32)
                    if flag is not None:
                        extra = extra + dead_lane * flag
                    swapped = pltpu.roll(extra, 64, 1)
                    low += [extra, swapped]
                    high += [swapped, extra]
                low = jnp.concatenate(low, axis=0).astype(jnp.bfloat16)
                high = jnp.concatenate(high, axis=0).astype(jnp.bfloat16)
                keys = nn(block[half, :HALF, :], key_w_ref[...]).astype(jnp.bfloat16)
                for head in range(HEADS):
                    column = keys[:, 128 * (head // 2) : 128 * (head // 2) + 128]
                    if head % 2 == 0:
                        full_key = jnp.where(low_lanes, column, high)
                    else:
                        full_key = jnp.where(low_lanes, low, column)
                    full_keys[head, at + HALF * half : at + HALF * half + HALF, :] = full_key
            rows = jnp.concatenate([block[0, :HALF, :], block[1, :HALF, :]], axis=0)
            every = nt(value_w_ref[...], rows).astype(jnp.bfloat16)
            for head in range(HEADS):
                values[bank, head, :64, at : at + ROWS] = every[64 * head : 64 * head + 64, :]

    def score(first, slot, keys_at, causal):
        for i in range(GROUP):
            head = first + i
            top = None
            for number in range(keys_at // HALF):
                at = HALF * number
                scores = nn(full_keys[head, at : at + HALF, :], query_ref[head])
                if causal:
                    key_at = lax.broadcasted_iota(jnp.int32, (HALF, ROWS), 0) + at
                    query_at = lax.broadcasted_iota(jnp.int32, (HALF, ROWS), 1)
                    scores = jnp.where(key_at <= query_at, scores, -MASKED)
                held[slot, i, at : at + HALF, :] = scores
                here = jnp.max(scores.reshape(HALF // 8, 8, ROWS), axis=0)
                top = here if top is None else jnp.maximum(top, here)
            tops[slot, i] = jnp.max(top, axis=0, keepdims=True)

    def weigh(first, slot, keys_at, causal):
        for i in range(GROUP):
            head = first + i
            if causal:
                new_max = tops[slot, i]
            else:
                old_max = run_max[head]
                new_max = jnp.maximum(old_max, tops[slot, i])
                factors[head] = jnp.exp2((old_max - new_max) * SCORE_BASE2)
            run_max[head] = new_max
            for number in range(keys_at // CHUNK):
                at = CHUNK * number
                probs[slot, i, at : at + CHUNK, :] = jnp.exp2(
                    (held[slot, i, at : at + CHUNK, :] - new_max) * SCORE_BASE2
                ).astype(jnp.bfloat16)

    def gather_values(first, slot, keys_at, bank, causal):
        for i in range(GROUP):
            head = first + i
            part = nn(values[bank, head, :, :keys_at], probs[slot, i, :keys_at, :])
            if causal:
                run_out[head] = part
            else:
                run_out[head] = run_out[head] * factors[head] + part

    project([own_ref], [None], 1)
    for j in range(GROUPS):
        score(j * GROUP, j % 2, ROWS, True)
        weigh(j * GROUP, j % 2, ROWS, True)
        gather_values(j * GROUP, j % 2, ROWS, 1, True)

    def pass_copy(kind, source):
        return remote(
            kv.at[kind, source, tp],
            kv.at[kind, source, tp],
            pass_send.at[kind, source],
            passed.at[kind, source],
            (sp, other),
        )

    def arrival(kind, source):
        return pltpu.make_async_copy(
            kv.at[kind, source, tp], kv.at[kind, source, tp], got.at[kind, source]
        )

    def take(origin):
        for kind in range(2):
            arrival(kind, origin).wait()
            pass_copy(kind, origin).start()

    def relay(j):
        origin = first_peer(-j)
        take(origin)

        @pl.when(tp == 1)
        def _():
            arrival(2, origin).wait()

        for k in (1, 3, 2):
            for kind in range(2):
                second_copy(kind, k, j).start()

    take(me)
    for k in (1, 3):
        for kind in range(2):
            first_copy(kind, k).start()
            second_copy(kind, k, 0).start()

    @pl.when(tp == 1)
    def _():
        for k in (1, 3):
            first_copy(2, k).start()

    for kind in range(2):
        first_copy(kind, 2).start()
        second_copy(kind, 2, 0).start()

    @pl.when(tp == 1)
    def _():
        first_copy(2, 2).start()

    for j in (1, 3):
        relay(j)
        take(second_peer(-j))

    pl.semaphore_wait(plane_in, DEPTH - 1)
    for k in range(1, DEPTH):
        pl.semaphore_signal(all_in, inc=1, device_id=in_line(0, k), device_id_type=MESH)

    last_slot = (GROUPS - 1) % 2
    last_head = (GROUPS - 1) * GROUP

    def errands(step):
        @pl.when(step == 0)
        def _():
            relay(2)
            take(second_peer(-2))

        for n in range(1, len(SEQUENCE) // 2 - 1):
            ahead = [o for o in SEQUENCE[2 * n + 2 : 2 * n + 4] if o[0] and o[1]]
            if ahead:

                @pl.when(step == n)
                def _(ahead=ahead):
                    for dy, dx in ahead:
                        take(place(-dy, -dx))

    def visit(step, carry):
        sources = []
        for i in range(2):
            dy, dx = 0, 0
            for n in range(len(SEQUENCE) // 2):
                dy = jnp.where(step == n, SEQUENCE[2 * n + i][0], dy)
                dx = jnp.where(step == n, SEQUENCE[2 * n + i][1], dx)
            sources.append(place(-dy, -dx))

        for source in sources:
            for kind in range(2):
                pltpu.make_async_copy(
                    kv.at[kind, source, other], kv.at[kind, source, other], passed.at[kind, source]
                ).wait()

        @pl.when(step >= 0)
        def _():
            bank = step % 2
            blocks, dead = [], []
            for source in sources:
                blocks += [kv.at[0, source], kv.at[1, source]]
                dead += [
                    (z < 1).astype(jnp.float32),
                    ((source >= me) & (z < 2)).astype(jnp.float32),
                ]

            project(blocks, dead, bank)
            score(0, 0, STEP, False)

            for j in range(GROUPS - 1):
                if j == 1:
                    errands(step)

                @pl.when(step >= -1 - j)
                def _(j=j):
                    if j > 0:
                        gather_values((j - 1) * GROUP, (j - 1) % 2, STEP, bank, False)
                    weigh(j * GROUP, j % 2, STEP, False)
                    score((j + 1) * GROUP, (j + 1) % 2, STEP, False)

            gather_values(last_head - GROUP, (last_slot + 1) % 2, STEP, bank, False)
            weigh(last_head, last_slot, STEP, False)
            gather_values(last_head, last_slot, STEP, bank, False)

        return carry

    lax.fori_loop(0, PLANE // 2, visit, 0)

    for head in range(HEADS):
        done = (run_out[head, :64, :] / run_out[head, 64:65, :]).astype(jnp.bfloat16)
        for part in range(2):
            turned_out[part, 64 * head : 64 * head + 64, :] = done[:, HALF * part : HALF * part + HALF]
    heads_copy = remote(
        turned_out.at[other], heads_buf.at[tp], heads_send, heads_got, (sp, other)
    )
    heads_copy.start()
    heads_buf[tp] = turned_out[tp]
    local_copies[0].wait()
    heads_copy.wait_recv()

    attended = jnp.concatenate(
        [heads_buf[g].astype(jnp.float32).T.astype(jnp.bfloat16) for g in range(2)], axis=1
    )
    squares = jnp.zeros((HALF, 1), jnp.float32)
    for n in range(4):
        cols = slice(512 * n, 512 * n + 512)
        part = nn(attended, proj[:, cols])
        mix[:, cols] = part
        squares = squares + jnp.sum(part * part, axis=1, keepdims=True)
    scale = lax.rsqrt(squares * (1.0 / D) + epsilon)
    squares = jnp.zeros((HALF, 1), jnp.float32)
    for n in range(4):
        cols = slice(512 * n, 512 * n + 512)
        branch = mix[:, cols] * scale * mix_gain_ref[:, cols]
        mid = (residual_ref[:, cols].astype(jnp.float32) + branch).astype(jnp.bfloat16)
        middle[:, cols] = mid
        wide = mid.astype(jnp.float32)
        squares = squares + jnp.sum(wide * wide, axis=1, keepdims=True)
    scale = lax.rsqrt(squares * (1.0 / D) + epsilon)
    for n in range(4):
        cols = slice(512 * n, 512 * n + 512)
        normed[:, cols] = (
            middle[:, cols].astype(jnp.float32) * scale * moe_gain_ref[:, cols]
        ).astype(jnp.bfloat16)

    at_row = lax.broadcasted_iota(jnp.int32, (HALF, HALF), 0)
    at_col = lax.broadcasted_iota(jnp.int32, (HALF, HALF), 1)
    expert_row = lax.broadcasted_iota(jnp.int32, (EXPERTS, HALF), 0)
    ids_t = ids_ref[...]
    hot = [(expert_row == ids_t[k : k + 1, :]).astype(jnp.float32) for k in range(2)]
    earlier = nn(
        (hot[0] + hot[1]).astype(jnp.bfloat16), (at_row < at_col).astype(jnp.float32).astype(jnp.bfloat16)
    )
    slot_row = lax.broadcasted_iota(jnp.int32, (EXPERTS * CAP, HALF), 0)
    chooser = jnp.zeros((EXPERTS * CAP, HALF), jnp.float32)
    for k in range(2):
        rank = jnp.sum(hot[k] * earlier, axis=0, keepdims=True).astype(jnp.int32)
        slot = ids_t[k : k + 1, :] * CAP + rank
        chooser = chooser + (slot_row == slot).astype(jnp.float32)
    chooser = chooser.astype(jnp.bfloat16)
    for n in range(8):
        cols = slice(256 * n, 256 * n + 256)
        picked = nn(chooser, normed[:, cols]).astype(jnp.bfloat16)
        send_buf[:, :, cols] = picked.reshape(EXPERTS, CAP, 256)

    def toward(offset, sign):
        dz, dy, dx = offset
        return (
            ((z + sign * dz + DEPTH) % DEPTH) * PLANE
            + ((y + sign * dy + DEPTH) % DEPTH) * DEPTH
            + (x + sign * dx + DEPTH) % DEPTH
        )

    def go_copy(kind, i):
        target = toward(ORDER[kind][i], 1)
        slot = kind * PLANE + i
        return remote(
            send_buf.at[target], recv_buf.at[slot], go_send.at[slot], go_got.at[slot], (target, tp)
        )

    def back_copy(kind, i):
        source = toward(ORDER[kind][i], -1)
        slot = kind * PLANE + i
        return remote(
            done_buf.at[slot], back_buf.at[sp], back_send.at[slot], back_got.at[sp], (source, tp)
        )

    pl.semaphore_wait(all_in, DEPTH - 1)
    away = [(kind, i) for kind in range(DEPTH) for i in range(PLANE) if any(ORDER[kind][i])]
    for kind, i in away:
        go_copy(kind, i).start()
    mine = pltpu.make_async_copy(send_buf.at[sp], recv_buf.at[OWN_SLOT], own_copy)
    mine.start()
    for copy in local_copies[1:]:
        copy.wait()
    for copy in weight_copies:
        copy.wait_recv()
    mine.wait()

    def expert_group(kind, carry):
        first = kind * PLANE
        rows = recv_buf[pl.ds(first, PLANE)].reshape(PLANE * CAP, D)
        hidden = []
        for half in range(2):
            gate_out = nn(rows, gate_w[half])
            up_out = nn(rows, up_w[half])
            hidden.append((gate_out / (1.0 + jnp.exp(-gate_out)) * up_out).astype(jnp.bfloat16))
        for n in range(4):
            cols = slice(512 * n, 512 * n + 512)
            parts = [
                nn(hidden[half], down_w[half, :, cols]).astype(jnp.bfloat16).astype(jnp.float32)
                for half in range(2)
            ]
            done_buf[pl.ds(first, PLANE), :, cols] = (
                (parts[0] + parts[1]).astype(jnp.bfloat16).reshape(PLANE, CAP, 512)
            )

    def turn(kind, carry):
        for k in range(DEPTH):

            @pl.when(kind == k)
            def _(k=k):
                for i in range(PLANE):
                    if any(ORDER[k][i]):
                        slot = k * PLANE + i
                        pltpu.make_async_copy(
                            recv_buf.at[slot], recv_buf.at[slot], go_got.at[slot]
                        ).wait()

        expert_group(kind, carry)
        for k in range(DEPTH):

            @pl.when(kind == k)
            def _(k=k):
                for i in range(PLANE):
                    if any(ORDER[k][i]):
                        back_copy(k, i).start()

        return carry

    lax.fori_loop(0, DEPTH, turn, 0)
    mine_back = pltpu.make_async_copy(done_buf.at[OWN_SLOT], back_buf.at[sp], own_copy)
    mine_back.start()

    expert_col = lax.broadcasted_iota(jnp.int32, (HALF, EXPERTS), 1)
    routes = [ids_t.astype(jnp.float32), route_ref[...], jnp.zeros((HALF - 4, HALF), jnp.float32)]
    routes = jnp.concatenate(routes, axis=0).T
    ids = routes[:, :2].astype(jnp.int32)
    hot = [(expert_col == ids[:, k : k + 1]).astype(jnp.float32) for k in range(2)]
    earlier = nn(
        (at_col < at_row).astype(jnp.float32).astype(jnp.bfloat16), (hot[0] + hot[1]).astype(jnp.bfloat16)
    )
    slot_col = lax.broadcasted_iota(jnp.int32, (HALF, EXPERTS * CAP), 1)
    takers = []
    for k in range(2):
        rank = jnp.sum(hot[k] * earlier, axis=1, keepdims=True).astype(jnp.int32)
        slot = ids[:, k : k + 1] * CAP + rank
        takers.append((slot_col == slot).astype(jnp.float32).astype(jnp.bfloat16))

    mine_back.wait()

    def await_back(step, carry):
        source = (sp + step) % EXPERTS
        pltpu.make_async_copy(
            back_buf.at[source], back_buf.at[source], back_got.at[source]
        ).wait()
        return carry

    lax.fori_loop(1, EXPERTS, await_back, 0)
    for n in range(4):
        cols = slice(512 * n, 512 * n + 512)
        came = back_buf[:, :, cols].reshape(EXPERTS * CAP, 512)
        both = (
            nn(takers[0], came) * routes[:, 2:3] + nn(takers[1], came) * routes[:, 3:4]
        )
        out_ref[:, cols] = (middle[:, cols].astype(jnp.float32) + both).astype(jnp.bfloat16)

    for copy in next_z:
        copy.wait_send()
    for copy in weight_copies:
        copy.wait_send()
    heads_copy.wait_send()

    for k in (1, 2, 3):
        for kind in range(2):
            first_copy(kind, k).wait_send()
            for j in range(DEPTH):
                second_copy(kind, k, j).wait_send()

        @pl.when(tp == 1)
        def _():
            first_copy(2, k).wait_send()

    def pass_done(source, carry):
        pass_copy(0, source).wait_send()
        pass_copy(1, source).wait_send()
        return carry

    lax.fori_loop(0, PLANE, pass_done, 0)

    for kind, i in away:
        go_copy(kind, i).wait_send()
        back_copy(kind, i).wait_send()


def local(
    residual,
    queries,
    latent,
    rope_key,
    doc_ids,
    latent_to_key,
    latent_to_value,
    out_proj,
    mix_gain,
    moe_gain,
    expert_ids,
    route_weight,
    gate_weight,
    up_weight,
    down_weight,
):
    bf16, f32 = jnp.bfloat16, jnp.float32
    first = lax.axis_index("sp") * ROWS
    positions = (first + jnp.arange(ROWS, dtype=jnp.int32)).astype(f32)
    half_width = ROPE // 2
    frequency = rope_base ** (-jnp.arange(half_width, dtype=f32) / half_width)
    angles = positions[None, :] * frequency[:, None]

    vmem = pl.BlockSpec(memory_space=pltpu.VMEM)
    anywhere = pl.BlockSpec(memory_space=pl.ANY)
    dma = pltpu.SemaphoreType.DMA
    return pl.pallas_call(
        kernel,
        out_shape=pltpu.VMEM((HALF, D), bf16),
        in_specs=[vmem] * 13 + [anywhere] * 4,
        out_specs=vmem,
        scratch_shapes=[
            pltpu.VMEM((2, PIECE, LATENT), bf16),
            pltpu.VMEM((HEADS, 128, ROWS), bf16),
            pltpu.VMEM((HEADS * 64, LATENT), bf16),
            pltpu.VMEM((3, PLANE, 2, PIECE, LATENT), bf16),
            pltpu.VMEM((HEADS, 1, ROWS), f32),
            pltpu.VMEM((2, GROUP, STEP, ROWS), f32),
            pltpu.VMEM((2, GROUP, 1, ROWS), f32),
            pltpu.VMEM((HEADS, 1, ROWS), f32),
            pltpu.VMEM((2, GROUP, STEP, ROWS), bf16),
            pltpu.VMEM((HEADS, STEP, 128), bf16),
            pltpu.VMEM((2, HEADS, 80, STEP), bf16),
            pltpu.VMEM((HEADS, 80, ROWS), f32),
            pltpu.VMEM((2, HEADS * 64, HALF), bf16),
            pltpu.VMEM((2, HEADS * 64, HALF), bf16),
            pltpu.VMEM((2 * HEADS * 64, D), bf16),
            pltpu.VMEM((2, D, FF_HALF), bf16),
            pltpu.VMEM((2, D, FF_HALF), bf16),
            pltpu.VMEM((2, FF_HALF, D), bf16),
            pltpu.VMEM((HALF, D), f32),
            pltpu.VMEM((HALF, D), bf16),
            pltpu.VMEM((HALF, D), bf16),
            pltpu.VMEM((EXPERTS, CAP, D), bf16),
            pltpu.VMEM((EXPERTS, CAP, D), bf16),
            pltpu.VMEM((EXPERTS, CAP, D), bf16),
            pltpu.VMEM((EXPERTS, CAP, D), bf16),
            dma((2,)),
            dma((3, DEPTH)),
            dma((2, DEPTH, DEPTH)),
            dma((2, PLANE)),
            dma((3, PLANE)),
            dma((2, PLANE)),
            dma((4,)),
            dma((3,)),
            dma((3,)),
            dma,
            dma,
            dma((EXPERTS,)),
            dma((EXPERTS,)),
            dma,
            dma((EXPERTS,)),
            dma((EXPERTS,)),
            pltpu.SemaphoreType.REGULAR,
            pltpu.SemaphoreType.REGULAR,
        ],
        compiler_params=pltpu.CompilerParams(
            collective_id=0, has_side_effects=True, vmem_limit_bytes=60 * 1024 * 1024
        ),
    )(
        queries.T,
        latent,
        rope_key.T,
        doc_ids.reshape(1, ROWS),
        jnp.cos(angles),
        jnp.sin(angles),
        latent_to_key,
        latent_to_value,
        residual,
        mix_gain.reshape(1, D),
        moe_gain.reshape(1, D),
        expert_ids.T,
        route_weight.T,
        out_proj,
        gate_weight,
        up_weight,
        down_weight,
    )


def solution(mesh):
    in_specs = (
        P(("sp", "tp"), None),
        P("sp", "tp"),
        P("sp", None),
        P("sp", None),
        P("sp"),
        P(None, "tp"),
        P(None, "tp"),
        P(),
        P(),
        P(),
        P(("sp", "tp"), None),
        P(("sp", "tp"), None),
        P("sp", None, "tp"),
        P("sp", None, "tp"),
        P("sp", "tp", None),
    )
    out_specs = P(("sp", "tp"), None)
    return jax.shard_map(local, mesh=mesh, in_specs=in_specs, out_specs=out_specs, check_vma=False)
```
